128 devices in a mesh: ep: 32 (over z, y, core), tp: 4 (over x).
Axes of the slice: x: 4, y: 4, z: 4, core: 2. Of those that a mesh axis runs over, the one named last changes fastest.
Arguments:
- mixer_input: bfloat16 [16384, 2048], P(('ep', 'tp')), may hold values from -6 to 6
- expert_input: bfloat16 [16384, 2048], P(('ep', 'tp')), may hold values from -6 to 6
- mixer_gain: float32 [2048], replicated, may hold values from 0.1 to 1.9
- query_down: bfloat16 [2048, 1536], replicated, may hold values from -0.125 to 0.125
- latent_down: bfloat16 [2048, 512], replicated, may hold values from -0.125 to 0.125
- rotary_down: bfloat16 [2048, 32], replicated, may hold values from -0.125 to 0.125
- query_gain: float32 [1536], replicated, may hold values from 0.8 to 40, as said below
- latent_gain: float32 [512], replicated, may hold values from 0.1 to 1.9
- query_plain: bfloat16 [1536, 1024], P(None, 'tp'), may hold values from -0.15625 to 0.15625
- query_rotary: bfloat16 [1536, 512], P(None, 'tp'), may hold values from -0.15625 to 0.15625
- key_plain: bfloat16 [512, 1024], P(None, 'tp'), may hold values from -0.25 to 0.25
- value_up: bfloat16 [512, 1024], P(None, 'tp'), may hold values from -0.25 to 0.25
- output_proj: bfloat16 [1024, 2048], P('tp'), may hold values from -0.1875 to 0.1875
- mixed_gain: float32 [2048], replicated, may hold values from 0.1 to 1.9
- expert_norm: float32 [2048], replicated, may hold values from 0.1 to 1.9
- route_ids: int32 [16384, 2], P(('ep', 'tp')), may hold values from 0 to 31, all different within a row; in each aligned block of 128 rows (0 to 127, 128 to 255, ...) at most 10 rows name the same one
- route_weight: float32 [16384, 2], P(('ep', 'tp')), may hold values from 0.2 to 1
- gate_proj: bfloat16 [32, 2048, 2048], P('ep', None, 'tp'), may hold values from -0.3984375 to 0.3984375
- up_proj: bfloat16 [32, 2048, 2048], P('ep', None, 'tp'), may hold values from -0.3984375 to 0.3984375
- down_proj: bfloat16 [32, 2048, 2048], P('ep', 'tp'), may hold values from -0.125 to 0.125
- expert_gain: float32 [2048], replicated, may hold values from 0.1 to 1.9
Outputs:
- mixer_out: bfloat16 [16384, 2048], P(('ep', 'tp'))
- expert_out: bfloat16 [16384, 2048], P(('ep', 'tp'))
The draws below stay inside these ranges and needn't reach their ends.
Inputs may be any that keep to these rules, and one draw needn't show every extreme that they name: `route_ids`: each row names 2 different experts. Within the rows of one device (128 aligned rows) no expert is named more than 10 times, a bound that some block reaches. `query_gain`: Positive.
All inputs are finite; a program needn't handle non-finite values.
Results may differ from the reference program's by a relative error of at most 0.018.
The reference program's roundings to bfloat16 on the way count: a program that leaves them out, or rounds other values in their place, can miss the bound.
Values may be sent and summed in bfloat16 or wider, within the bound.
A program may use at most 128 MiB of HBM per device.

```python
import math
import jax
import jax.numpy as jnp
import numpy as np
from jax import lax

D = 2048
HEADS = 16
NOPE = 64
ROPE = 32
VDIM = 64
Q_RANK = 1536
KV_RANK = 512
FF = 2048
TOPK = 2
TOK_DEV = 128
TOKENS = 16384
EXPERTS = 32
CAP = 10
N_TP = 4


def draw_query_gain(key, part):
    return 1.0 + 0.18 * jax.random.uniform(key, (Q_RANK,), jnp.float32, -1.0, 1.0)


def steps_of(rng, shape, pieces, low, largest):
    loudness = 1.0
    for dim, parts in pieces:
        steps = jax.random.uniform(jax.random.fold_in(jax.random.fold_in(rng, 6), dim), (parts,), jnp.float32, low / len(pieces), largest / len(pieces))
        loudness = loudness * jnp.repeat(jnp.exp(steps), shape[dim] // parts).reshape((-1,) + (1,) * (len(shape) - 1 - dim))
    return loudness


def shared_out(rng, own, number, rows, amount, top, reach, skew):
    ranking = jax.random.permutation(rng, amount)
    packed, ordinary = shares(amount, rows * top, reach, skew, True), shares(amount, rows * top, reach, skew, False)
    places = jnp.arange(amount)

    def named(tallies, rotation):
        used = int((tallies > 0).sum())
        fixed = max(1, used // 4)
        passed = fixed + (places - fixed + rotation * (used - fixed)) % max(1, amount - fixed)
        return jnp.zeros((amount,), jnp.int32).at[ranking[jnp.where(places < fixed, places, passed)]].set(jnp.asarray(tallies, jnp.int32))

    tallies = jnp.where(number % 4 == 0, named(packed, number // 4), named(ordinary, number - number // 4 - 1))
    mixed = jax.random.permutation(jax.random.fold_in(own, 3), amount)
    donor, receiver = mixed[0:amount // 2 * 2:2], mixed[1:amount // 2 * 2:2]
    margin = jnp.minimum(tallies[donor] - 1, reach - tallies[receiver]) // 2
    margin = jnp.where((donor == ranking[0]) | (receiver == ranking[0]) | (tallies[receiver] == 0), 0, jnp.maximum(margin, 0))
    passed = jax.random.randint(jax.random.fold_in(own, 4), (amount // 2,), 0, 1 << 20) % (margin + 1)
    tallies = tallies.at[donor].add(-passed).at[receiver].add(passed)
    members = jnp.searchsorted(jnp.cumsum(tallies), jnp.arange(rows * top), side="right").astype(jnp.int32)
    grid = members.reshape(top, rows).T
    grid = grid[jax.random.permutation(jax.random.fold_in(own, 1), rows)]
    rotation = jax.random.randint(jax.random.fold_in(own, 2), (rows, 1), 0, top)
    return jnp.take_along_axis(grid, (jnp.arange(top)[None, :] + rotation) % top, axis=1)


def shares(count, total, most, slope, full):
    portions = [(1 << 20) // math.isqrt(rank ** slope) + 1 for rank in range(1, count + 1)]
    largest = most if full else min(most, max(-(-total // count), total * portions[0] // sum(portions)))
    least = 1 if total - largest >= count - 1 else 0
    holding, spare = [largest] + [least] * (count - 1), total - largest - least * (count - 1)
    while spare > 0:
        movable = [i for i in range(1, count) if holding[i] < largest] or [i for i in range(1, count) if holding[i] < most]
        mass, remaining = sum([portions[i] for i in movable]), spare
        for i in movable:
            more = min(most - holding[i], max(1, remaining * portions[i] // mass), spare)
            holding[i] = holding[i] + more
            spare = spare - more
    return np.array(holding)


def normal_values(key, extent, deviation, most, pieces=(), held_as=jnp.bfloat16):
    values = deviation * jax.random.normal(key, extent, jnp.float32)
    if pieces:
        values = values * steps_of(key, extent, pieces, -0.22, 0.18)
    return jnp.clip(values, -most, most).astype(held_as)


def setup_inputs(seed: int = 0) -> dict:
    streams_of = jax.random.split(jax.random.key(seed), 22)
    mixer_input = normal_values(streams_of[0], (TOKENS, D), 1.0, 6.0, ((0, 128),))
    expert_input = normal_values(streams_of[1], (TOKENS, D), 1.0, 6.0, ((0, 128),))
    mixer_gain = jnp.clip(1.0 + 0.18 * jax.random.normal(streams_of[2], (D,), jnp.float32), 0.1, 1.9)
    query_down = normal_values(streams_of[3], (D, Q_RANK), D ** -0.5, 0.125)
    latent_down = normal_values(streams_of[4], (D, KV_RANK), D ** -0.5, 0.125)
    rotary_down = normal_values(streams_of[5], (D, ROPE), D ** -0.5, 0.125)
    query_gain = draw_query_gain(jax.random.fold_in(streams_of[21], 71), 0)
    latent_gain = jnp.clip(1.0 + 0.18 * jax.random.normal(streams_of[7], (KV_RANK,), jnp.float32), 0.1, 1.9)
    query_plain = normal_values(streams_of[8], (Q_RANK, HEADS * NOPE), Q_RANK ** -0.5, 0.15625, ((1, 4),))
    query_rotary = normal_values(streams_of[9], (Q_RANK, HEADS * ROPE), Q_RANK ** -0.5, 0.15625, ((1, 4),))
    key_plain = normal_values(streams_of[10], (KV_RANK, HEADS * NOPE), KV_RANK ** -0.5, 0.25, ((1, 4),))
    value_up = normal_values(streams_of[11], (KV_RANK, HEADS * VDIM), KV_RANK ** -0.5, 0.25, ((1, 4),))
    output_proj = normal_values(streams_of[12], (HEADS * VDIM, D), (HEADS * VDIM) ** -0.5, 0.1875, ((0, 4),))
    mixed_gain = jnp.clip(1.0 + 0.18 * jax.random.normal(streams_of[13], (D,), jnp.float32), 0.1, 1.9)
    expert_norm = jnp.clip(1.0 + 0.18 * jax.random.normal(streams_of[14], (D,), jnp.float32), 0.1, 1.9)
    route_ids_keys = jax.random.split(jax.random.fold_in(streams_of[15], 1), TOKENS // TOK_DEV)
    route_ids_turns = jax.random.permutation(jax.random.fold_in(streams_of[15], 3), TOKENS // TOK_DEV)
    route_ids = jax.vmap(lambda own, number: shared_out(jax.random.fold_in(streams_of[15], 2), own, number, TOK_DEV, EXPERTS, TOPK, CAP, 0))(route_ids_keys, route_ids_turns).reshape((TOKENS, TOPK))
    route_weight = jnp.clip(jnp.exp(math.log(1.0) - 1.609438 * jax.random.uniform(streams_of[16], (TOKENS, TOPK), jnp.float32) ** steps_of(streams_of[16], (TOKENS, TOPK), ((0, 128),), -0.2, 0.2)), 0.2, 1.0)
    gate_proj = normal_values(streams_of[17], (EXPERTS, D, FF), 0.066, 0.3984375, ((0, 32), (2, 4)))
    up_proj = normal_values(streams_of[18], (EXPERTS, D, FF), 0.066, 0.3984375, ((0, 32), (2, 4)))
    down_proj = normal_values(streams_of[19], (EXPERTS, FF, D), FF ** -0.5, 0.125, ((0, 32), (1, 4)))
    expert_gain = jnp.clip(1.0 + 0.18 * jax.random.normal(streams_of[20], (D,), jnp.float32), 0.1, 1.9)
    return {"mixer_input": mixer_input, "expert_input": expert_input, "mixer_gain": mixer_gain, "query_down": query_down, "latent_down": latent_down, "rotary_down": rotary_down, "query_gain": query_gain, "latent_gain": latent_gain, "query_plain": query_plain, "query_rotary": query_rotary, "key_plain": key_plain, "value_up": value_up, "output_proj": output_proj, "mixed_gain": mixed_gain, "expert_norm": expert_norm, "route_ids": route_ids, "route_weight": route_weight, "gate_proj": gate_proj, "up_proj": up_proj, "down_proj": down_proj, "expert_gain": expert_gain}


EPS = 1e-06
CLAMP = 7.0
ALPHA = 1.702
THETA = 10000.0

def norm_rows(values, gain):
    values = values.astype(jnp.float32)
    scale = lax.rsqrt(lax.optimization_barrier(jnp.mean(values * values, axis=-1, keepdims=True)) + EPS)
    return values * scale * gain.astype(jnp.float32)

def rounded(values):
    return lax.optimization_barrier(values.astype(jnp.bfloat16)).astype(jnp.float32)

def turn_tables(positions, width):
    half = width // 2
    freqs = THETA ** (-2.0 * jnp.arange(half, dtype=jnp.float32) / width)
    angles = positions.astype(jnp.float32)[:, None] * freqs[None, :]
    return (jnp.cos(angles), jnp.sin(angles))

def rotate(values, cosine, sine):
    half = values.shape[-1] // 2
    first = values[..., :half]
    second = values[..., half:]
    return jnp.concatenate([first * cosine - second * sine, second * cosine + first * sine], axis=-1)

def reference(mixer_input, expert_input, mixer_gain, query_down, latent_down, rotary_down, query_gain, latent_gain, query_plain, query_rotary, key_plain, value_up, output_proj, mixed_gain, expert_norm, route_ids, route_weight, gate_proj, up_proj, down_proj, expert_gain):
    positions = jnp.arange(TOKENS, dtype=jnp.int32)
    hidden = norm_rows(mixer_input, mixer_gain).astype(jnp.bfloat16)
    query_lat = norm_rows(jnp.dot(hidden, query_down, preferred_element_type=jnp.float32), query_gain).astype(jnp.bfloat16)
    key_lat = norm_rows(jnp.dot(hidden, latent_down, preferred_element_type=jnp.float32), latent_gain).astype(jnp.bfloat16)
    cosine, sine = turn_tables(positions, ROPE)
    key_turn = rotate(jnp.dot(hidden, rotary_down, preferred_element_type=jnp.float32), cosine, sine).astype(jnp.bfloat16)
    query_nope = jnp.dot(query_lat, query_plain, preferred_element_type=jnp.float32).astype(jnp.bfloat16).reshape(TOKENS, HEADS, NOPE)
    query_pe = rotate(jnp.dot(query_lat, query_rotary, preferred_element_type=jnp.float32).reshape(TOKENS, HEADS, ROPE), cosine[:, None, :], sine[:, None, :]).astype(jnp.bfloat16)
    keys = rounded(jnp.dot(key_lat, key_plain, preferred_element_type=jnp.float32)).reshape(TOKENS, HEADS, NOPE)
    values = rounded(jnp.dot(key_lat, value_up, preferred_element_type=jnp.float32)).reshape(TOKENS, HEADS, VDIM)
    turned = key_turn.astype(jnp.float32)
    scale = (NOPE + ROPE) ** (-0.5)
    span = math.gcd(TOKENS, 128)

    def attend(block):
        plain, rotated = block
        scores = (jnp.einsum('qhd,khd->qhk', plain.astype(jnp.float32), keys) + jnp.einsum('qhr,kr->qhk', rotated.astype(jnp.float32), turned)) * scale
        peak = lax.optimization_barrier(jnp.max(scores, axis=-1, keepdims=True))
        expos = jnp.exp(scores - peak)
        totals = lax.optimization_barrier(jnp.sum(expos, axis=-1))
        summed = jnp.einsum('qhk,khd->qhd', rounded(expos), values)
        return (summed / totals[..., None]).astype(jnp.bfloat16)
    attended = lax.map(attend, (query_nope.reshape(TOKENS // span, span, HEADS, NOPE), query_pe.reshape(TOKENS // span, span, HEADS, ROPE)))
    attended = attended.reshape(TOKENS, HEADS * VDIM)
    width = HEADS * VDIM // N_TP
    mixed = jnp.zeros((TOKENS, D), jnp.float32)
    for group in range(N_TP):
        mixed = mixed + rounded(jnp.dot(attended[:, group * width:(group + 1) * width], output_proj[group * width:(group + 1) * width], preferred_element_type=jnp.float32))
    mixer_out = norm_rows(mixed, mixed_gain).astype(jnp.bfloat16)
    expert_hidden = norm_rows(expert_input, expert_norm).astype(jnp.bfloat16)
    blocks = TOKENS // TOK_DEV
    assigned = TOK_DEV * TOPK
    block_ids = route_ids.reshape(blocks, assigned)
    onehot = (block_ids[:, :, None] == jnp.arange(EXPERTS, dtype=jnp.int32)[None, None, :]).astype(jnp.int32)
    order = lax.optimization_barrier(jnp.sum((jnp.cumsum(onehot, axis=1) - onehot) * onehot, axis=2))
    slot = (jnp.arange(blocks, dtype=jnp.int32)[:, None] * CAP + order).reshape(-1).astype(jnp.int32)
    owner = (jnp.arange(blocks * assigned, dtype=jnp.int32) // TOPK).astype(jnp.int32)
    flat_ids = route_ids.reshape(-1).astype(jnp.int32)
    table = jnp.zeros((EXPERTS, blocks * CAP), jnp.int32).at[flat_ids, slot].set(owner)
    share = jnp.zeros((EXPERTS, blocks * CAP), jnp.float32).at[flat_ids, slot].set(route_weight.reshape(-1).astype(jnp.float32))
    units = FF // N_TP

    def one_expert(total, inputs):
        rows_at, weight_at, gate_w, up_w, down_w = inputs
        rows = expert_hidden[rows_at]
        gate = jnp.minimum(jnp.dot(rows, gate_w, preferred_element_type=jnp.float32), CLAMP)
        up = jnp.clip(jnp.dot(rows, up_w, preferred_element_type=jnp.float32), -CLAMP, CLAMP)
        act = ((up + 1.0) * gate * jax.nn.sigmoid(ALPHA * gate)).astype(jnp.bfloat16)
        result = jnp.zeros((rows.shape[0], D), jnp.float32)
        for group in range(N_TP):
            result = result + rounded(jnp.dot(act[:, group * units:(group + 1) * units], down_w[group * units:(group + 1) * units], preferred_element_type=jnp.float32))
        result = rounded(result)
        total = total.at[rows_at].add(result * weight_at[:, None])
        return (total, None)
    combined, _ = lax.scan(one_expert, jnp.zeros((TOKENS, D), jnp.float32), (table, share, gate_proj, up_proj, down_proj))
    expert_out = norm_rows(combined, expert_gain).astype(jnp.bfloat16)
    return (mixer_out, expert_out)
```

```python
import functools

import jax
import jax.numpy as jnp
from jax import lax
from jax.experimental import pallas as pl
from jax.experimental.pallas import tpu as pltpu
from jax.sharding import PartitionSpec as P

NOPE = 64
ROPE = 32
VDIM = 64


EPS = 1e-06
CLAMP = 7.0
ALPHA = 1.702
THETA = 10000.0
FLOOR = -1e30
LOG2E = 1.4426950408889634
C = (NOPE + ROPE) ** (-0.5) * LOG2E
SUB = 128

def attend_kernel(heads, qn_ref, qt_ref, kv_ref, o_ref, rhs, s_buf, p_buf, peak, acc):
    step = pl.program_id(0)
    pair, size = kv_ref.shape[0], kv_ref.shape[2]
    subs = size // SUB
    wide = heads * NOPE
    rows = pair * SUB
    queries = qn_ref.shape[1]

    @pl.when(step == 0)
    def _():
        rhs[...] = jnp.zeros_like(rhs)
        for h in range(heads):
            for j in range(subs):
                at = h % 2 * NOPE
                rhs[h, j, at : at + NOPE, :] = qn_ref[h * NOPE : (h + 1) * NOPE, :]
                low = 128 + j * ROPE
                rhs[h, j, low : low + ROPE, :] = qt_ref[h * ROPE : (h + 1) * ROPE, :]
        peak[...] = jnp.full_like(peak, -1e30)
        acc[...] = jnp.zeros_like(acc)

    turned = jnp.concatenate(
        [
            kv_ref[b, 2 * wide :, g * 128 : (g + 1) * 128]
            for b in range(pair)
            for g in range(size // 128)
        ],
        axis=0,
    )

    def scores(h):
        half = wide // SUB
        best = None
        for j in range(subs):
            left = jnp.concatenate(
                [
                    kv_ref[
                        b,
                        j % half * SUB : (j % half + 1) * SUB,
                        j // half * wide + h // 2 * 128 : j // half * wide + h // 2 * 128 + 128,
                    ]
                    for b in range(pair)
                ],
                axis=0,
            )
            left = jnp.concatenate([left, turned], axis=1)
            part = jnp.dot(left, rhs[h, j], preferred_element_type=jnp.float32)
            s_buf[h % 2, j * rows : (j + 1) * rows, :] = part
            top = jnp.max(part.reshape(rows // 8, 8, queries), axis=0)
            best = top if best is None else jnp.maximum(best, top)
        return jnp.max(best, axis=0, keepdims=True)

    def finish(h, best):
        old = peak[h : h + 1, :]
        new = jnp.maximum(old, best)
        peak[h : h + 1, :] = new
        shrink = jnp.exp2((old - new) * C)
        base = new * C
        for j in range(subs):
            at = slice(j * rows, (j + 1) * rows)
            p_buf[h % 2, at, :] = jnp.exp2(s_buf[h % 2, at, :] * C - base).astype(jnp.bfloat16)
        left = jnp.concatenate(
            [
                kv_ref[b, wide + h * VDIM : wide + (h + 1) * VDIM, j * SUB : (j + 1) * SUB]
                for j in range(subs)
                for b in range(pair)
            ],
            axis=1,
        )
        left = jnp.concatenate([left, jnp.ones((16, left.shape[1]), jnp.bfloat16)], axis=0)
        more = jnp.dot(left, p_buf[h % 2], preferred_element_type=jnp.float32)
        acc[h] = acc[h] * shrink + more

    best = scores(0)
    for h in range(heads):
        later = scores(h + 1) if h + 1 < heads else None
        finish(h, best)
        best = later

    @pl.when(step == pl.num_programs(0) - 1)
    def _():
        for h in range(heads):
            o_ref[h * VDIM : (h + 1) * VDIM, :] = (
                acc[h, :VDIM, :] / acc[h, VDIM : VDIM + 1, :]
            ).astype(jnp.bfloat16)


def attend(qn, qt, packed, pair=2):
    heads = qn.shape[0] // NOPE
    queries = qn.shape[1]
    blocks, height, size = packed.shape
    subs = size // SUB
    return pl.pallas_call(
        functools.partial(attend_kernel, heads),
        out_shape=jax.ShapeDtypeStruct((heads * VDIM, queries), jnp.bfloat16),
        grid=(blocks // pair,),
        in_specs=[
            pl.BlockSpec(qn.shape, lambda i: (0, 0)),
            pl.BlockSpec(qt.shape, lambda i: (0, 0)),
            pl.BlockSpec((pair, height, size), lambda i: (i, 0, 0)),
        ],
        out_specs=pl.BlockSpec((heads * VDIM, queries), lambda i: (0, 0)),
        scratch_shapes=[
            pltpu.VMEM((heads, subs, 256, queries), jnp.bfloat16),
            pltpu.VMEM((2, pair * size, queries), jnp.float32),
            pltpu.VMEM((2, pair * size, queries), jnp.bfloat16),
            pltpu.VMEM((8, queries), jnp.float32),
            pltpu.VMEM((heads, VDIM + 16, queries), jnp.float32),
        ],
        compiler_params=pltpu.CompilerParams(
            dimension_semantics=("arbitrary",), vmem_limit_bytes=56 * 1024 * 1024
        ),
        cost_estimate=pl.CostEstimate(
            flops=2 * heads * queries * blocks * size * (256 + VDIM),
            bytes_accessed=blocks * height * size * 2,
            transcendentals=heads * queries * blocks * size,
        ),
    )(qn, qt, packed)


def in_one_piece(arrays, axis, dim, along):
    widths = [a.shape[along] for a in arrays]
    both = jnp.concatenate(arrays, axis=along)
    out = lax.all_gather(both, axis, axis=dim, tiled=True)
    return tuple(jnp.split(out, [sum(widths[:k]) for k in range(1, len(widths))], axis=along))


def split_up(shard, dim, peers):
    before, after = (shard.shape[:dim], shard.shape[dim + 1 :])
    return jnp.moveaxis(shard.reshape(*before, peers, -1, *after), dim, 0)


def summed_on_arrival(shard, axis, dim):
    blocks = split_up(shard, dim, lax.axis_size(axis))
    arrived = lax.all_to_all(blocks, axis, split_axis=0, concat_axis=0, tiled=True)
    return arrived.astype(jnp.float32).sum(axis=0)


def norm_rows(values, gain):
    values = values.astype(jnp.float32)
    scale = lax.rsqrt(jnp.mean(values * values, axis=-1, keepdims=True) + EPS)
    return values * scale * gain


def turn_tables(positions, width):
    half = width // 2
    freqs = THETA ** (-2.0 * jnp.arange(half, dtype=jnp.float32) / width)
    angles = positions.astype(jnp.float32)[:, None] * freqs[None, :]
    return (jnp.cos(angles), jnp.sin(angles))


def rotate(values, cosine, sine):
    half = values.shape[-1] // 2
    first = values[..., :half]
    second = values[..., half:]
    return jnp.concatenate(
        [first * cosine - second * sine, second * cosine + first * sine], axis=-1
    )


def on_device(
    mixer_input,
    expert_input,
    mixer_gain,
    query_down,
    latent_down,
    rotary_down,
    query_gain,
    latent_gain,
    query_plain,
    query_rotary,
    key_plain,
    value_up,
    output_proj,
    mixed_gain,
    expert_norm,
    route_ids,
    route_weight,
    gate_proj,
    up_proj,
    down_proj,
    expert_gain,
):
    tok_rows = mixer_input.shape[0]
    groups = lax.axis_size("tp")
    group_base = lax.axis_index("ep") * groups * tok_rows
    offset = group_base + lax.axis_index("tp") * tok_rows
    heads_here = query_plain.shape[1] // NOPE
    hidden = norm_rows(mixer_input, mixer_gain).astype(jnp.bfloat16)
    query_lat = norm_rows(
        jnp.dot(hidden, query_down, preferred_element_type=jnp.float32), query_gain
    ).astype(jnp.bfloat16)
    key_lat = norm_rows(
        jnp.dot(hidden, latent_down, preferred_element_type=jnp.float32), latent_gain
    ).astype(jnp.bfloat16)
    cosine, sine = turn_tables(offset + jnp.arange(tok_rows, dtype=jnp.int32), ROPE)
    key_turn = rotate(
        jnp.dot(hidden, rotary_down, preferred_element_type=jnp.float32), cosine, sine
    ).astype(jnp.bfloat16)
    collected = in_one_piece((query_lat, key_lat), "tp", 0, 1)
    turned = lax.all_gather(key_turn, "tp", axis=1, tiled=True)
    qlat, latents = collected
    count = qlat.shape[0]
    across = (((0,), (1,)), ((), ()))
    qn = lax.dot_general(query_plain, qlat, across, preferred_element_type=jnp.float32).astype(
        jnp.bfloat16
    )
    rotated = lax.dot_general(query_rotary, qlat, across, preferred_element_type=jnp.float32)
    rotated = rotated.reshape(heads_here, 2, ROPE // 2, count)
    all_cos, all_sin = turn_tables(group_base + jnp.arange(count, dtype=jnp.int32), ROPE)
    all_cos, all_sin = all_cos.T[None], all_sin.T[None]
    first, second = rotated[:, 0], rotated[:, 1]
    qt = (
        jnp.concatenate(
            [first * all_cos - second * all_sin, second * all_cos + first * all_sin], axis=1
        )
        .astype(jnp.bfloat16)
        .reshape(heads_here * ROPE, count)
    )
    keys = jnp.dot(latents, key_plain, preferred_element_type=jnp.float32).astype(jnp.bfloat16)
    values = lax.dot_general(value_up, latents, across, preferred_element_type=jnp.float32).astype(
        jnp.bfloat16
    )
    half = heads_here * NOPE
    keys = jnp.concatenate([keys[g * half : (g + 1) * half] for g in range(count // half)], axis=1)
    strips = tok_rows * turned.shape[1] // count
    turned = jnp.concatenate(
        [turned[g * strips : (g + 1) * strips] for g in range(tok_rows // strips)], axis=1
    )
    packed = jnp.concatenate([keys, values, turned], axis=0)
    packed = lax.all_gather(packed, "ep", axis=0, tiled=False)
    attended = attend(qn, qt, packed)
    mixed = summed_on_arrival(
        lax.dot_general(
            attended, output_proj, (((0,), (0,)), ((), ())), preferred_element_type=jnp.float32
        ).astype(jnp.bfloat16),
        "tp",
        0,
    )
    mixer_out = norm_rows(mixed, mixed_gain).astype(jnp.bfloat16)
    expert_hidden = norm_rows(expert_input, expert_norm).astype(jnp.bfloat16)
    experts = lax.axis_size("ep")
    topk = route_ids.shape[1]
    capacity = 5 * tok_rows * topk // (4 * experts)
    slots = experts * capacity
    flat_ids = route_ids.reshape(-1)
    onehot = (flat_ids[:, None] == jnp.arange(experts, dtype=jnp.int32)[None, :]).astype(jnp.int32)
    order = jnp.sum((jnp.cumsum(onehot, axis=0) - onehot) * onehot, axis=1)
    target = flat_ids * capacity + order
    dispatch = jnp.any(
        target.reshape(tok_rows, topk)[None, :, :]
        == jnp.arange(slots, dtype=jnp.int32)[:, None, None],
        axis=2,
    ).astype(jnp.bfloat16)
    outgoing = (
        jnp.dot(dispatch, expert_hidden, preferred_element_type=jnp.float32)
        .astype(jnp.bfloat16)
        .reshape(experts, capacity, expert_hidden.shape[1])
    )
    gate_w = gate_proj[0]
    up_w = up_proj[0]
    down_w = down_proj[0]
    received = lax.all_to_all(outgoing, "ep", split_axis=0, concat_axis=0, tiled=True)
    sources, count, width = received.shape
    rows = received.reshape(sources * count, width)
    piece = lax.all_gather(rows, "tp", axis=0, tiled=True)
    gate = jnp.minimum(jnp.dot(piece, gate_w, preferred_element_type=jnp.float32), CLAMP)
    up = jnp.clip(jnp.dot(piece, up_w, preferred_element_type=jnp.float32), -CLAMP, CLAMP)
    acts = ((up + 1.0) * gate * jax.nn.sigmoid(ALPHA * gate)).astype(jnp.bfloat16)
    sums = summed_on_arrival(
        jnp.dot(acts, down_w, preferred_element_type=jnp.float32).astype(jnp.bfloat16), "tp", 0
    )
    returned = sums.astype(jnp.bfloat16).reshape(sources, count, width)
    back_rows = lax.all_to_all(returned, "ep", split_axis=0, concat_axis=0, tiled=True).reshape(
        slots, expert_hidden.shape[1]
    )
    picked = back_rows[target].astype(jnp.float32).reshape(tok_rows, topk, expert_hidden.shape[1])
    combined = jnp.sum(picked * route_weight[:, :, None], axis=1)
    expert_out = norm_rows(combined, expert_gain).astype(jnp.bfloat16)
    return (mixer_out, expert_out)


def solution(mesh):
    in_specs = (
        P(("ep", "tp"), None),
        P(("ep", "tp"), None),
        P(),
        P(),
        P(),
        P(),
        P(),
        P(),
        P(None, "tp"),
        P(None, "tp"),
        P(None, "tp"),
        P(None, "tp"),
        P("tp", None),
        P(),
        P(),
        P(("ep", "tp"), None),
        P(("ep", "tp"), None),
        P("ep", None, "tp"),
        P("ep", None, "tp"),
        P("ep", "tp", None),
        P(),
    )
    out_specs = (P(("ep", "tp"), None), P(("ep", "tp"), None))
    return jax.shard_map(
        on_device, mesh=mesh, in_specs=in_specs, out_specs=out_specs, check_vma=False
    )
```

```python
import functools

import jax
import jax.numpy as jnp
from jax import lax
from jax.experimental import pallas as pl
from jax.experimental.pallas import tpu as pltpu
from jax.sharding import PartitionSpec as P

NOPE = 64
ROPE = 32
VDIM = 64


EPS = 1e-06
CLAMP = 7.0
ALPHA = 1.702
THETA = 10000.0
FLOOR = -1e30
LOG2E = 1.4426950408889634
C = (NOPE + ROPE) ** (-0.5) * LOG2E
SUB = 128

MESH = pl.DeviceIdType.MESH
ANY = pl.BlockSpec(memory_space=pl.ANY)
VMEM = pl.BlockSpec(memory_space=pltpu.VMEM)
DMA = pltpu.SemaphoreType.DMA


def ring_places():
    ep, tp, n = lax.axis_index("ep"), lax.axis_index("tp"), lax.axis_size("tp")
    right = lax.rem(tp + 1, n)
    left = lax.rem(tp + n - 1, n)
    across = lax.rem(tp + 2, n)
    return ep, tp, right, left, across


def partner(ep, r):
    for bit in range(r.bit_length()):
        if r >> bit & 1:
            ep = ep + (1 - 2 * lax.rem(ep // (1 << bit), 2)) * (1 << bit)
    return ep


def greet(places):
    barrier = pltpu.get_barrier_semaphore()
    for place in places:
        pl.semaphore_signal(barrier, inc=1, device_id=place, device_id_type=MESH)
    pl.semaphore_wait(barrier, len(places))


def remote(src, dst, sends, recvs, k, place):
    return pltpu.make_async_remote_copy(
        src_ref=src,
        dst_ref=dst,
        send_sem=sends.at[k],
        recv_sem=recvs.at[k],
        device_id=place,
        device_id_type=MESH,
    )


def exchange_kernel(latent_count, *refs):
    lats, rows = refs[:latent_count], refs[latent_count]
    outs, rows_out = refs[latent_count + 1 : 2 * latent_count + 1], refs[2 * latent_count + 1]
    kept, kept_rows = refs[2 * latent_count + 2 : 3 * latent_count + 2], refs[3 * latent_count + 2]
    own_sem, sends, recvs, row_sends, row_recvs = refs[3 * latent_count + 3 :]
    ep, tp, right, left, across = ring_places()
    peers = rows.shape[0]
    swaps = [(partner(ep, r), tp) for r in range(1, peers)]
    to_right, to_left = (ep, right), (ep, left)
    greet(swaps + [to_right, to_left])
    own = [
        pltpu.make_async_copy(src, dst, own_sem.at[k])
        for k, (src, dst) in enumerate(
            [(a, b) for a, b in zip(lats, kept)] + [(rows.at[0], kept_rows)]
        )
    ]
    first, second, waits = [], [], []
    for k, (lat, out) in enumerate(zip(lats, outs)):
        half = lat.shape[0] // 2
        for part, place in ((0, to_right), (1, to_left), (1, to_right), (0, to_left)):
            way = 0 if place is to_right else 1
            at = pl.ds(part * half, half)
            first.append(
                remote(
                    lat.at[at], out.at[tp, at], sends, recvs, 6 * k + 2 * way + part, place
                )
            )
        for way, place, origin in ((0, to_right, left), (1, to_left, right)):
            at = pl.ds(way * half, half)
            second.append(
                remote(
                    out.at[origin, at], out.at[origin, at], sends, recvs, 6 * k + 4 + way, place
                )
            )
    moves = [
        remote(rows.at[r], rows_out.at[r], row_sends, row_recvs, r - 1, swaps[r - 1])
        for r in range(1, peers)
    ]
    for copy in first:
        copy.start()
    for copy in moves:
        copy.start()
    for copy in own:
        copy.start()
    for copy in own:
        copy.wait()
    back = [
        pltpu.make_async_copy(src, dst, own_sem.at[k])
        for k, (src, dst) in enumerate(
            [(a, b.at[tp]) for a, b in zip(kept, outs)] + [(kept_rows, rows_out.at[0])]
        )
    ]
    for copy in back:
        copy.start()
    for k in range(latent_count):
        first[4 * k].wait_recv()
        second[2 * k].start()
        first[4 * k + 1].wait_recv()
        second[2 * k + 1].start()
    for k in range(latent_count):
        first[4 * k + 2].wait_recv()
        first[4 * k + 3].wait_recv()
    for copy in second:
        copy.wait_recv()
    for copy in moves:
        copy.wait_recv()
    for copy in first + second + moves:
        copy.wait_send()
    for copy in back:
        copy.wait()


def exchange(lats, rows):
    groups = lax.axis_size("tp")
    count = len(lats)
    peers = rows.shape[0]
    return pl.pallas_call(
        functools.partial(exchange_kernel, count),
        out_shape=[jax.ShapeDtypeStruct((groups, *a.shape), a.dtype) for a in lats]
        + [jax.ShapeDtypeStruct(rows.shape, rows.dtype)],
        in_specs=[ANY] * (count + 1),
        out_specs=[ANY] * (count + 1),
        scratch_shapes=[pltpu.VMEM(a.shape, a.dtype) for a in lats]
        + [
            pltpu.VMEM(rows.shape[1:], rows.dtype),
            DMA((count + 1,)),
            DMA((6 * count,)),
            DMA((6 * count,)),
            DMA((peers - 1,)),
            DMA((peers - 1,)),
        ],
        compiler_params=pltpu.CompilerParams(
            collective_id=1, has_side_effects=True, vmem_limit_bytes=8 * 1024 * 1024
        ),
        cost_estimate=pl.CostEstimate(flops=10**10, bytes_accessed=10**6, transcendentals=0),
    )(*lats, rows)


def gather_kernel(x, out, kept, own_sem, sends, recvs):
    ep, tp, right, left, across = ring_places()
    to_right, to_left = (ep, right), (ep, left)
    greet([to_right, to_left])
    size = x.shape[0] // 4

    def chunk(c):
        return pl.ds(c * size, size)

    def fresh(c, way):
        return remote(
            x.at[chunk(c)], out.at[tp, chunk(c)], sends, recvs, 4 * way + c, (to_right, to_left)[way]
        )

    def onward(c):
        way = c // 2
        origin = (left, right)[way]
        part = out.at[origin, chunk(c)]
        return remote(part, part, sends, recvs, 8 + c, (to_right, to_left)[way])

    news = {(c, way): fresh(c, way) for c in range(4) for way in range(2)}
    passed = [onward(c) for c in range(4)]
    for key in ((0, 0), (2, 1), (1, 0), (3, 1)):
        news[key].start()
    take = pltpu.make_async_copy(x, kept, own_sem.at[0])
    take.start()
    take.wait()
    put = pltpu.make_async_copy(kept, out.at[tp], own_sem.at[0])
    put.start()
    for c in range(2):
        news[c, 0].wait_recv()
        passed[c].start()
        news[2 + c, 0].start()
        news[2 + c, 1].wait_recv()
        passed[2 + c].start()
        news[c, 1].start()
    for c in range(2):
        news[2 + c, 0].wait_recv()
        news[c, 1].wait_recv()
    for copy in passed:
        copy.wait_recv()
    for copy in passed + list(news.values()):
        copy.wait_send()
    put.wait()


def gather_rows(x):
    groups = lax.axis_size("tp")
    return pl.pallas_call(
        gather_kernel,
        out_shape=jax.ShapeDtypeStruct((groups, *x.shape), x.dtype),
        in_specs=[ANY],
        out_specs=ANY,
        scratch_shapes=[pltpu.VMEM(x.shape, x.dtype), DMA((1,)), DMA((12,)), DMA((12,))],
        compiler_params=pltpu.CompilerParams(
            collective_id=2, has_side_effects=True, vmem_limit_bytes=8 * 1024 * 1024
        ),
        cost_estimate=pl.CostEstimate(flops=10**10, bytes_accessed=10**6, transcendentals=0),
    )(x)


class Fold:
    def __init__(self, part, far, near, mixed, sends, recvs):
        self.part, self.far, self.near, self.mixed = part, far, near, mixed
        ep, tp, right, left, across = ring_places()
        self.tp, self.sides = tp, (right, left)
        self.places = ((ep, right), (ep, left))
        self.size = size = part.shape[1] // 4
        self.at = [pl.ds(c * size, size) for c in range(4)]
        self.hops = []
        self.plain = []
        self.joined = []
        for c in range(4):
            way = c // 2
            other = 1 - way
            self.hops.append(
                remote(part.at[across, self.at[c]], far.at[c], sends, recvs, c, self.places[way])
            )
            self.plain.append(
                remote(
                    part.at[self.sides[other], self.at[c]],
                    near.at[c],
                    sends,
                    recvs,
                    4 + c,
                    self.places[other],
                )
            )
            self.joined.append(
                remote(mixed.at[c], far.at[4 + c], sends, recvs, 8 + c, self.places[way])
            )

    def open(self):
        greet(list(self.places))
        for c in (0, 2, 1, 3):
            self.hops[c].start()
        for c in (2, 0, 3, 1):
            self.plain[c].start()

    def join(self, c):
        own = self.part[self.sides[c // 2], self.at[c], :]
        self.mixed[c] = (own.astype(jnp.float32) + self.far[c].astype(jnp.float32)).astype(
            jnp.bfloat16
        )

    def total(self, c):
        self.joined[c].wait_recv()
        own = self.part[self.tp, self.at[c], :].astype(jnp.float32)
        return own + self.near[c].astype(jnp.float32) + self.far[4 + c].astype(jnp.float32)

    def close(self):
        for copy in self.hops + self.plain + self.joined:
            copy.wait_send()


def fold_scratch(rows, width):
    return [
        pltpu.VMEM((8, rows // 4, width), jnp.bfloat16),
        pltpu.VMEM((4, rows // 4, width), jnp.bfloat16),
        pltpu.VMEM((4, rows // 4, width), jnp.bfloat16),
        DMA((12,)),
        DMA((12,)),
    ]


def finish_kernel(part, gain, rows, out, rows_out, kept, own_sem, far, near, mixed, sends, recvs, row_sends, row_recvs):
    ep, tp, right, left, across = ring_places()
    peers = rows.shape[0]
    swaps = [(partner(ep, r), tp) for r in range(1, peers)]
    barrier = pltpu.get_barrier_semaphore()
    for place in swaps:
        pl.semaphore_signal(barrier, inc=1, device_id=place, device_id_type=MESH)
    fold = Fold(part, far, near, mixed, sends, recvs)
    for place in fold.places:
        pl.semaphore_signal(barrier, inc=1, device_id=place, device_id_type=MESH)
    pl.semaphore_wait(barrier, len(swaps) + 2)
    for c in (0, 2, 1, 3):
        fold.hops[c].start()
    for c in (2, 0, 3, 1):
        fold.plain[c].start()
    moves = [
        remote(rows.at[r], rows_out.at[r], row_sends, row_recvs, r - 1, swaps[r - 1])
        for r in range(1, peers)
    ]
    for copy in moves:
        copy.start()
    take = pltpu.make_async_copy(rows.at[0], kept, own_sem.at[0])
    take.start()
    take.wait()
    put = pltpu.make_async_copy(kept, rows_out.at[0], own_sem.at[0])
    put.start()
    for c in (0, 2):
        fold.hops[c].wait_recv()
        fold.join(c)
    for c in (1, 3):
        fold.hops[c].wait_recv()
    for c in (0, 2):
        fold.joined[c].start()
    for c in (1, 3):
        fold.join(c)
    for c in (0, 2):
        fold.plain[c].wait_recv()
    for c in (1, 3):
        fold.joined[c].start()
        fold.plain[c].wait_recv()
    for c in range(4):
        whole = fold.total(c)
        scale = lax.rsqrt(jnp.mean(whole * whole, axis=-1, keepdims=True) + EPS)
        out[fold.at[c], :] = (whole * scale * gain[...]).astype(jnp.bfloat16)
    fold.close()
    for copy in moves:
        copy.wait()
    put.wait()


def finish(part, gain, rows):
    groups, count, width = part.shape
    peers = rows.shape[0]
    return pl.pallas_call(
        finish_kernel,
        out_shape=[
            jax.ShapeDtypeStruct((count, width), jnp.bfloat16),
            jax.ShapeDtypeStruct(rows.shape, rows.dtype),
        ],
        in_specs=[VMEM, VMEM, ANY],
        out_specs=[VMEM, ANY],
        scratch_shapes=[pltpu.VMEM(rows.shape[1:], rows.dtype), DMA((1,))]
        + fold_scratch(count, width)
        + [DMA((peers - 1,)), DMA((peers - 1,))],
        compiler_params=pltpu.CompilerParams(
            collective_id=3, has_side_effects=True, vmem_limit_bytes=16 * 1024 * 1024
        ),
        cost_estimate=pl.CostEstimate(flops=10**10, bytes_accessed=10**6, transcendentals=0),
    )(part, gain.reshape(1, width), rows)


def attend_kernel(
    heads, qn_ref, qt_ref, kv_ref, part, o_ref, sum_ref, rhs, s_buf, p_buf, peak, acc, *fold_refs
):
    step = pl.program_id(0)
    steps = pl.num_programs(0)
    fold = Fold(part, *fold_refs)

    @pl.when(step == 0)
    def _():
        fold.open()

    @pl.when(step == steps * 5 // 16)
    def _():
        for c in range(4):
            fold.hops[c].wait_recv()
            fold.join(c)

    @pl.when(step == steps * 5 // 16 + 1)
    def _():
        for c in (0, 2, 1, 3):
            fold.joined[c].start()

    pair, size = kv_ref.shape[0], kv_ref.shape[2]
    subs = size // SUB
    wide = heads * NOPE
    rows = pair * SUB
    queries = qn_ref.shape[1]

    @pl.when(step == 0)
    def _():
        rhs[...] = jnp.zeros_like(rhs)
        for h in range(heads):
            for j in range(subs):
                at = h % 2 * NOPE
                rhs[h, j, at : at + NOPE, :] = qn_ref[h * NOPE : (h + 1) * NOPE, :]
                low = 128 + j * ROPE
                rhs[h, j, low : low + ROPE, :] = qt_ref[h * ROPE : (h + 1) * ROPE, :]
        peak[...] = jnp.full_like(peak, -1e30)
        acc[...] = jnp.zeros_like(acc)

    turned = jnp.concatenate(
        [
            kv_ref[b, 2 * wide :, g * 128 : (g + 1) * 128]
            for b in range(pair)
            for g in range(size // 128)
        ],
        axis=0,
    )

    def scores(h):
        half = wide // SUB
        best = None
        for j in range(subs):
            left = jnp.concatenate(
                [
                    kv_ref[
                        b,
                        j % half * SUB : (j % half + 1) * SUB,
                        j // half * wide + h // 2 * 128 : j // half * wide + h // 2 * 128 + 128,
                    ]
                    for b in range(pair)
                ],
                axis=0,
            )
            left = jnp.concatenate([left, turned], axis=1)
            part = jnp.dot(left, rhs[h, j], preferred_element_type=jnp.float32)
            s_buf[h % 2, j * rows : (j + 1) * rows, :] = part
            top = jnp.max(part.reshape(rows // 8, 8, queries), axis=0)
            best = top if best is None else jnp.maximum(best, top)
        return jnp.max(best, axis=0, keepdims=True)

    def finish(h, best):
        old = peak[h : h + 1, :]
        new = jnp.maximum(old, best)
        peak[h : h + 1, :] = new
        shrink = jnp.exp2((old - new) * C)
        base = new * C
        for j in range(subs):
            at = slice(j * rows, (j + 1) * rows)
            p_buf[h % 2, at, :] = jnp.exp2(s_buf[h % 2, at, :] * C - base).astype(jnp.bfloat16)
        left = jnp.concatenate(
            [
                kv_ref[b, wide + h * VDIM : wide + (h + 1) * VDIM, j * SUB : (j + 1) * SUB]
                for j in range(subs)
                for b in range(pair)
            ],
            axis=1,
        )
        left = jnp.concatenate([left, jnp.ones((16, left.shape[1]), jnp.bfloat16)], axis=0)
        more = jnp.dot(left, p_buf[h % 2], preferred_element_type=jnp.float32)
        acc[h] = acc[h] * shrink + more

    best = scores(0)
    for h in range(heads):
        later = scores(h + 1) if h + 1 < heads else None
        finish(h, best)
        best = later

    @pl.when(step == steps - 1)
    def _():
        for c in range(4):
            fold.plain[c].wait_recv()
            sum_ref[fold.at[c], :] = fold.total(c).astype(jnp.bfloat16)
        fold.close()
        for h in range(heads):
            o_ref[h * VDIM : (h + 1) * VDIM, :] = (
                acc[h, :VDIM, :] / acc[h, VDIM : VDIM + 1, :]
            ).astype(jnp.bfloat16)


def attend(qn, qt, packed, part, pair=2):
    heads = qn.shape[0] // NOPE
    queries = qn.shape[1]
    blocks, height, size = packed.shape
    subs = size // SUB
    return pl.pallas_call(
        functools.partial(attend_kernel, heads),
        out_shape=[
            jax.ShapeDtypeStruct((heads * VDIM, queries), jnp.bfloat16),
            jax.ShapeDtypeStruct(part.shape[1:], jnp.bfloat16),
        ],
        grid=(blocks // pair,),
        in_specs=[
            pl.BlockSpec(qn.shape, lambda i: (0, 0)),
            pl.BlockSpec(qt.shape, lambda i: (0, 0)),
            pl.BlockSpec((pair, height, size), lambda i: (i, 0, 0)),
            VMEM,
        ],
        out_specs=[
            pl.BlockSpec((heads * VDIM, queries), lambda i: (0, 0)),
            pl.BlockSpec(part.shape[1:], lambda i: (0, 0)),
        ],
        scratch_shapes=[
            pltpu.VMEM((heads, subs, 256, queries), jnp.bfloat16),
            pltpu.VMEM((2, pair * size, queries), jnp.float32),
            pltpu.VMEM((2, pair * size, queries), jnp.bfloat16),
            pltpu.VMEM((8, queries), jnp.float32),
            pltpu.VMEM((heads, VDIM + 16, queries), jnp.float32),
        ]
        + fold_scratch(part.shape[1], part.shape[2]),
        compiler_params=pltpu.CompilerParams(
            dimension_semantics=("arbitrary",),
            vmem_limit_bytes=56 * 1024 * 1024,
            collective_id=4,
            has_side_effects=True,
        ),
        cost_estimate=pl.CostEstimate(
            flops=2 * heads * queries * blocks * size * (256 + VDIM),
            bytes_accessed=blocks * height * size * 2,
            transcendentals=heads * queries * blocks * size,
        ),
    )(qn, qt, packed, part)


def norm_rows(values, gain):
    values = values.astype(jnp.float32)
    scale = lax.rsqrt(jnp.mean(values * values, axis=-1, keepdims=True) + EPS)
    return values * scale * gain


def turn_tables(positions, width):
    half = width // 2
    freqs = THETA ** (-2.0 * jnp.arange(half, dtype=jnp.float32) / width)
    angles = positions.astype(jnp.float32)[:, None] * freqs[None, :]
    return (jnp.cos(angles), jnp.sin(angles))


def rotate(values, cosine, sine):
    half = values.shape[-1] // 2
    first = values[..., :half]
    second = values[..., half:]
    return jnp.concatenate(
        [first * cosine - second * sine, second * cosine + first * sine], axis=-1
    )


def on_device(
    mixer_input,
    expert_input,
    mixer_gain,
    query_down,
    latent_down,
    rotary_down,
    query_gain,
    latent_gain,
    query_plain,
    query_rotary,
    key_plain,
    value_up,
    output_proj,
    mixed_gain,
    expert_norm,
    route_ids,
    route_weight,
    gate_proj,
    up_proj,
    down_proj,
    expert_gain,
):
    tok_rows = mixer_input.shape[0]
    groups = lax.axis_size("tp")
    group_base = lax.axis_index("ep") * groups * tok_rows
    offset = group_base + lax.axis_index("tp") * tok_rows
    heads_here = query_plain.shape[1] // NOPE
    hidden = norm_rows(mixer_input, mixer_gain).astype(jnp.bfloat16)
    query_lat = norm_rows(
        jnp.dot(hidden, query_down, preferred_element_type=jnp.float32), query_gain
    ).astype(jnp.bfloat16)
    key_lat = norm_rows(
        jnp.dot(hidden, latent_down, preferred_element_type=jnp.float32), latent_gain
    ).astype(jnp.bfloat16)
    cosine, sine = turn_tables(offset + jnp.arange(tok_rows, dtype=jnp.int32), ROPE)
    key_turn = rotate(
        jnp.dot(hidden, rotary_down, preferred_element_type=jnp.float32), cosine, sine
    ).astype(jnp.bfloat16)
    expert_hidden = norm_rows(expert_input, expert_norm).astype(jnp.bfloat16)
    experts = lax.axis_size("ep")
    topk = route_ids.shape[1]
    capacity = 5 * tok_rows * topk // (4 * experts)
    slots = experts * capacity
    flat_ids = route_ids.reshape(-1)
    onehot = (flat_ids[:, None] == jnp.arange(experts, dtype=jnp.int32)[None, :]).astype(jnp.int32)
    order = jnp.sum((jnp.cumsum(onehot, axis=0) - onehot) * onehot, axis=1)
    target = (flat_ids ^ lax.axis_index("ep")) * capacity + order
    dispatch = jnp.any(
        target.reshape(tok_rows, topk)[None, :, :]
        == jnp.arange(slots, dtype=jnp.int32)[:, None, None],
        axis=2,
    ).astype(jnp.bfloat16)
    outgoing = (
        jnp.dot(dispatch, expert_hidden, preferred_element_type=jnp.float32)
        .astype(jnp.bfloat16)
        .reshape(experts, capacity, expert_hidden.shape[1] // 128, 128)
    )
    wide_turn = jnp.pad(key_turn, ((0, 0), (0, 128 - ROPE)))
    latents, turned, qlat, received = exchange((key_lat, wide_turn, query_lat), outgoing)
    count = groups * tok_rows
    latents = latents.reshape(count, latents.shape[2])
    qlat = qlat.reshape(count, qlat.shape[2])
    turned = jnp.concatenate([turned[g, :, :ROPE] for g in range(groups)], axis=1)
    across = (((0,), (1,)), ((), ()))
    qn = lax.dot_general(query_plain, qlat, across, preferred_element_type=jnp.float32).astype(
        jnp.bfloat16
    )
    rotated = lax.dot_general(query_rotary, qlat, across, preferred_element_type=jnp.float32)
    rotated = rotated.reshape(heads_here, 2, ROPE // 2, count)
    all_cos, all_sin = turn_tables(group_base + jnp.arange(count, dtype=jnp.int32), ROPE)
    all_cos, all_sin = all_cos.T[None], all_sin.T[None]
    first, second = rotated[:, 0], rotated[:, 1]
    qt = (
        jnp.concatenate(
            [first * all_cos - second * all_sin, second * all_cos + first * all_sin], axis=1
        )
        .astype(jnp.bfloat16)
        .reshape(heads_here * ROPE, count)
    )
    keys = jnp.dot(latents, key_plain, preferred_element_type=jnp.float32).astype(jnp.bfloat16)
    values = lax.dot_general(value_up, latents, across, preferred_element_type=jnp.float32).astype(
        jnp.bfloat16
    )
    half = heads_here * NOPE
    keys = jnp.concatenate([keys[g * half : (g + 1) * half] for g in range(count // half)], axis=1)
    strips = tok_rows * turned.shape[1] // count
    turned = jnp.concatenate(
        [turned[g * strips : (g + 1) * strips] for g in range(tok_rows // strips)], axis=1
    )
    packed = jnp.concatenate([keys, values, turned], axis=0)
    packed = lax.all_gather(packed, "ep", axis=0, tiled=False)
    gate_w = gate_proj[0]
    up_w = up_proj[0]
    down_w = down_proj[0]
    width = expert_hidden.shape[1]
    piece = gather_rows(received.reshape(slots, width)).reshape(groups * slots, width)
    gate = jnp.minimum(jnp.dot(piece, gate_w, preferred_element_type=jnp.float32), CLAMP)
    up = jnp.clip(jnp.dot(piece, up_w, preferred_element_type=jnp.float32), -CLAMP, CLAMP)
    acts = ((up + 1.0) * gate * jax.nn.sigmoid(ALPHA * gate)).astype(jnp.bfloat16)
    part = jnp.dot(acts, down_w, preferred_element_type=jnp.float32).astype(jnp.bfloat16)
    attended, sums = attend(qn, qt, packed, part.reshape(groups, slots, width))
    mixed = lax.dot_general(
        attended, output_proj, (((0,), (0,)), ((), ())), preferred_element_type=jnp.float32
    ).astype(jnp.bfloat16)
    mixer_out, back_rows = finish(
        mixed.reshape(groups, tok_rows, width),
        mixed_gain,
        sums.reshape(experts, capacity, width // 128, 128),
    )
    back_rows = back_rows.reshape(slots, width // 128, 128)
    picked = back_rows[target].astype(jnp.float32).reshape(tok_rows, topk, width // 128, 128)
    combined = jnp.sum(picked * route_weight[:, :, None, None], axis=1).reshape(tok_rows, width)
    expert_out = norm_rows(combined, expert_gain).astype(jnp.bfloat16)
    return (mixer_out, expert_out)


def solution(mesh):
    in_specs = (
        P(("ep", "tp"), None),
        P(("ep", "tp"), None),
        P(),
        P(),
        P(),
        P(),
        P(),
        P(),
        P(None, "tp"),
        P(None, "tp"),
        P(None, "tp"),
        P(None, "tp"),
        P("tp", None),
        P(),
        P(),
        P(("ep", "tp"), None),
        P(("ep", "tp"), None),
        P("ep", None, "tp"),
        P("ep", None, "tp"),
        P("ep", "tp", None),
        P(),
    )
    out_specs = (P(("ep", "tp"), None), P(("ep", "tp"), None))
    return jax.shard_map(
        on_device, mesh=mesh, in_specs=in_specs, out_specs=out_specs, check_vma=False
    )
```

```python
import functools

import jax
import jax.numpy as jnp
from jax import lax
from jax.experimental import pallas as pl
from jax.experimental.pallas import tpu as pltpu
from jax.sharding import PartitionSpec as P

NOPE = 64
ROPE = 32
VDIM = 64


EPS = 1e-06
CLAMP = 7.0
ALPHA = 1.702
THETA = 10000.0
FLOOR = -1e30
LOG2E = 1.4426950408889634
C = (NOPE + ROPE) ** (-0.5) * LOG2E
SUB = 64

MESH = pl.DeviceIdType.MESH
ANY = pl.BlockSpec(memory_space=pl.ANY)
VMEM = pl.BlockSpec(memory_space=pltpu.VMEM)
DMA = pltpu.SemaphoreType.DMA


def ring_places():
    ep, tp, n = lax.axis_index("ep"), lax.axis_index("tp"), lax.axis_size("tp")
    right = lax.rem(tp + 1, n)
    left = lax.rem(tp + n - 1, n)
    across = lax.rem(tp + 2, n)
    return ep, tp, right, left, across


def partner(ep, r):
    for bit in range(r.bit_length()):
        if r >> bit & 1:
            ep = ep + (1 - 2 * lax.rem(ep // (1 << bit), 2)) * (1 << bit)
    return ep


def greet(places):
    barrier = pltpu.get_barrier_semaphore()
    for place in places:
        pl.semaphore_signal(barrier, inc=1, device_id=place, device_id_type=MESH)
    pl.semaphore_wait(barrier, len(places))


def remote(src, dst, sends, recvs, k, place):
    return pltpu.make_async_remote_copy(
        src_ref=src,
        dst_ref=dst,
        send_sem=sends.at[k],
        recv_sem=recvs.at[k],
        device_id=place,
        device_id_type=MESH,
    )


def exchange_kernel(latent_count, *refs):
    lats, rows = refs[:latent_count], refs[latent_count]
    outs, rows_out = refs[latent_count + 1 : 2 * latent_count + 1], refs[2 * latent_count + 1]
    kept, kept_rows = refs[2 * latent_count + 2 : 3 * latent_count + 2], refs[3 * latent_count + 2]
    own_sem, sends, recvs, row_sends, row_recvs = refs[3 * latent_count + 3 :]
    ep, tp, right, left, across = ring_places()
    peers = rows.shape[0]
    swaps = [(partner(ep, r), tp) for r in range(1, peers)]
    to_right, to_left = (ep, right), (ep, left)
    greet(swaps + [to_right, to_left])
    own = [
        pltpu.make_async_copy(src, dst, own_sem.at[k])
        for k, (src, dst) in enumerate(
            [(a, b) for a, b in zip(lats, kept)] + [(rows.at[0], kept_rows)]
        )
    ]
    first, second, waits = [], [], []
    for k, (lat, out) in enumerate(zip(lats, outs)):
        half = lat.shape[0] // 2
        for part, place in ((0, to_right), (1, to_left), (1, to_right), (0, to_left)):
            way = 0 if place is to_right else 1
            at = pl.ds(part * half, half)
            first.append(
                remote(
                    lat.at[at], out.at[tp, at], sends, recvs, 6 * k + 2 * way + part, place
                )
            )
        for way, place, origin in ((0, to_right, left), (1, to_left, right)):
            at = pl.ds(way * half, half)
            second.append(
                remote(
                    out.at[origin, at], out.at[origin, at], sends, recvs, 6 * k + 4 + way, place
                )
            )
    moves = [
        remote(rows.at[r], rows_out.at[r], row_sends, row_recvs, r - 1, swaps[r - 1])
        for r in range(1, peers)
    ]
    for copy in first:
        copy.start()
    for copy in moves:
        copy.start()
    for copy in own:
        copy.start()
    for copy in own:
        copy.wait()
    back = [
        pltpu.make_async_copy(src, dst, own_sem.at[k])
        for k, (src, dst) in enumerate(
            [(a, b.at[tp]) for a, b in zip(kept, outs)] + [(kept_rows, rows_out.at[0])]
        )
    ]
    for copy in back:
        copy.start()
    for k in range(latent_count):
        first[4 * k].wait_recv()
        second[2 * k].start()
        first[4 * k + 1].wait_recv()
        second[2 * k + 1].start()
    for k in range(latent_count):
        first[4 * k + 2].wait_recv()
        first[4 * k + 3].wait_recv()
    for copy in second:
        copy.wait_recv()
    for copy in moves:
        copy.wait_recv()
    for copy in first + second + moves:
        copy.wait_send()
    for copy in back:
        copy.wait()


def exchange(lats, rows):
    groups = lax.axis_size("tp")
    count = len(lats)
    peers = rows.shape[0]
    return pl.pallas_call(
        functools.partial(exchange_kernel, count),
        out_shape=[jax.ShapeDtypeStruct((groups, *a.shape), a.dtype) for a in lats]
        + [jax.ShapeDtypeStruct(rows.shape, rows.dtype)],
        in_specs=[ANY] * (count + 1),
        out_specs=[ANY] * (count + 1),
        scratch_shapes=[pltpu.VMEM(a.shape, a.dtype) for a in lats]
        + [
            pltpu.VMEM(rows.shape[1:], rows.dtype),
            DMA((count + 1,)),
            DMA((6 * count,)),
            DMA((6 * count,)),
            DMA((peers - 1,)),
            DMA((peers - 1,)),
        ],
        compiler_params=pltpu.CompilerParams(
            collective_id=1, has_side_effects=True, vmem_limit_bytes=8 * 1024 * 1024
        ),
        cost_estimate=pl.CostEstimate(flops=10**10, bytes_accessed=10**6, transcendentals=0),
    )(*lats, rows)


class Spread:
    def __init__(self, own, held, sends, recvs):
        ep, tp = lax.axis_index("ep"), lax.axis_index("tp")
        side = 4
        core = lax.rem(ep, 2)
        y = lax.rem(ep // 2, side)
        z = ep // (2 * side)
        self.own, self.held, self.sends, self.recvs = own, held, sends, recvs
        self.ep, self.tp = ep, tp
        self.mate = ep + 1 - 2 * core
        cut = held.shape[2] // 32 * 16
        self.parts = (pl.ds(0, cut), pl.ds(cut, held.shape[2] - cut))

        def index(dz, dy):
            return (lax.rem(z + dz, side) * side + lax.rem(y + dy, side)) * 2 + core

        self.block = lambda f, a, b: index(b, a) if f == 0 else index(a, b)
        self.neighbours = [index(1, 0), index(3, 0), index(0, 1), index(0, 3)]

    def place(self, f, ring, way):
        step = (1, 3)[way]
        return (self.block(f, step, 0) if ring == 0 else self.block(f, 0, step), self.tp)

    def copy(self, f, a, b, place, k, part=None):
        mine = a == 0 and b == 0
        where = self.block(f, a, b)
        if part is None:
            src = self.own.at[f] if mine else self.held.at[where, f]
            dst = self.held.at[where, f]
        else:
            src = self.held.at[where, f, self.parts[part]]
            dst = src
        return remote(src, dst, self.sends, self.recvs, 36 * f + k, place)

    def first(self, f, way):
        return self.copy(f, 0, 0, self.place(f, 0, way), way)

    def first_on(self, f, way):
        return self.copy(f, (3, 1)[way], 0, self.place(f, 0, way), 2 + way, part=way)

    def second(self, f, a, way):
        return self.copy(f, a, 0, self.place(f, 1, way), 4 + 4 * a + way)

    def second_on(self, f, a, way):
        return self.copy(f, a, (3, 1)[way], self.place(f, 1, way), 6 + 4 * a + way, part=way)

    def share(self, f, a, b):
        return self.copy(f, a, b, (self.mate, self.tp), 20 + 4 * a + b)

    def everyone(self):
        return [(place, self.tp) for place in self.neighbours] + [(self.mate, self.tp)]

    def start(self):
        for f in range(2):
            for way in range(2):
                self.first(f, way).start()
        for f in range(2):
            self.share(f, 0, 0).start()
            for way in range(2):
                self.second(f, 0, way).start()

    def got_first(self):
        for f in range(2):
            for way in range(2):
                self.first(f, way).wait_recv()
                self.first_on(f, way).start()
                a = (3, 1)[way]
                for there in range(2):
                    self.second(f, a, there).start()
                self.share(f, a, 0).start()

    def got_second(self, a):
        for f in range(2):
            for way in range(2):
                self.second(f, a, way).wait_recv()
                self.second_on(f, a, way).start()
                self.share(f, a, (3, 1)[way]).start()

    def got_far_first(self):
        for f in range(2):
            for way in range(2):
                self.first_on(f, way).wait_recv()
            for there in range(2):
                self.second(f, 2, there).start()
            self.share(f, 2, 0).start()

    def got_far_second(self, a):
        for f in range(2):
            for way in range(2):
                self.second_on(f, a, way).wait_recv()
            self.share(f, a, 2).start()

    def close(self):
        for f in range(2):
            for a in range(4):
                for b in range(4):
                    self.share(f, a, b).wait()
            for way in range(2):
                self.first(f, way).wait_send()
                self.first_on(f, way).wait_send()
                for a in range(4):
                    self.second(f, a, way).wait_send()
                    self.second_on(f, a, way).wait_send()


def gather_kernel(
    x,
    latents,
    key_plain,
    value_up,
    turned,
    qlat,
    query_plain,
    query_rotary,
    cosine,
    sine,
    out,
    held,
    qn,
    qt,
    kept,
    block,
    own_sem,
    sends,
    recvs,
    kv_sends,
    kv_recvs,
):
    ep, tp, right, left, across = ring_places()
    to_right, to_left = (ep, right), (ep, left)
    size = x.shape[0] // 4
    spread = Spread(block, held, kv_sends, kv_recvs)
    barrier = pltpu.get_barrier_semaphore()
    places = [to_right, to_left] + spread.everyone()
    for place in places:
        pl.semaphore_signal(barrier, inc=1, device_id=place, device_id_type=MESH)
    take = pltpu.make_async_copy(x, kept, own_sem.at[0])
    take.start()

    keys = jnp.dot(latents[...], key_plain[...], preferred_element_type=jnp.float32)
    values = jnp.dot(latents[...], value_up[...], preferred_element_type=jnp.float32).T
    keys, values = keys.astype(jnp.bfloat16), values.astype(jnp.bfloat16)
    low = keys.shape[1]
    half = low // 2
    for f in range(2):
        block[f, :half, :low] = keys[low * f : low * f + half]
        block[f, :half, low:] = keys[low * f + half : low * f + low]
        block[f, half:low, :low] = values[:half, low * f : low * f + low]
        block[f, half:low, low:] = values[half:, low * f : low * f + low]
        block[f, low:, :] = turned[f]
    take.wait()
    put = pltpu.make_async_copy(kept, out.at[tp], own_sem.at[0])
    put.start()
    pl.semaphore_wait(barrier, len(places))

    def chunk(c):
        return pl.ds(c * size, size)

    def fresh(c, way):
        return remote(
            x.at[chunk(c)], out.at[tp, chunk(c)], sends, recvs, 4 * way + c, (to_right, to_left)[way]
        )

    def onward(c):
        way = c // 2
        origin = (left, right)[way]
        part = out.at[origin, chunk(c)]
        return remote(part, part, sends, recvs, 8 + c, (to_right, to_left)[way])

    news = {(c, way): fresh(c, way) for c in range(4) for way in range(2)}
    passed = [onward(c) for c in range(4)]
    for key in ((0, 0), (2, 1), (1, 0), (3, 1)):
        news[key].start()
    spread.start()
    keep = pltpu.make_async_copy(block, held.at[ep], own_sem.at[1])
    keep.start()

    plain = jnp.dot(qlat[...], query_plain[...], preferred_element_type=jnp.float32)
    qn[...] = plain.T.astype(jnp.bfloat16)
    rotated = jnp.dot(qlat[...], query_rotary[...], preferred_element_type=jnp.float32).T
    quarter = ROPE // 2
    for h in range(rotated.shape[0] // ROPE):
        a = rotated[h * ROPE : h * ROPE + quarter]
        b = rotated[h * ROPE + quarter : h * ROPE + ROPE]
        qt[h * ROPE : h * ROPE + quarter, :] = (a * cosine[...] - b * sine[...]).astype(
            jnp.bfloat16
        )
        qt[h * ROPE + quarter : h * ROPE + ROPE, :] = (b * cosine[...] + a * sine[...]).astype(
            jnp.bfloat16
        )

    def pass_rows(c):
        news[c, 0].wait_recv()
        passed[c].start()
        news[2 + c, 0].start()
        news[2 + c, 1].wait_recv()
        passed[2 + c].start()
        news[c, 1].start()

    spread.got_first()
    pass_rows(0)
    spread.got_second(0)
    pass_rows(1)
    spread.got_far_first()
    spread.got_second(3)
    spread.got_second(1)
    spread.got_far_second(0)
    spread.got_second(2)
    for a in (3, 1, 2):
        spread.got_far_second(a)
    spread.close()
    for c in range(2):
        news[2 + c, 0].wait_recv()
        news[c, 1].wait_recv()
    for copy in passed:
        copy.wait_recv()
    for copy in passed + list(news.values()):
        copy.wait_send()
    put.wait()
    keep.wait()


def gather(x, latents, key_plain, value_up, turned, qlat, query_plain, query_rotary, cosine, sine):
    groups, peers = lax.axis_size("tp"), lax.axis_size("ep")
    count = latents.shape[0]
    low = key_plain.shape[1]
    height = low + turned.shape[1]
    wide = turned.shape[2]
    return pl.pallas_call(
        gather_kernel,
        out_shape=[
            jax.ShapeDtypeStruct((groups, *x.shape), x.dtype),
            jax.ShapeDtypeStruct((peers, 2, height, wide), x.dtype),
            jax.ShapeDtypeStruct((query_plain.shape[1], count), x.dtype),
            jax.ShapeDtypeStruct((query_rotary.shape[1], count), x.dtype),
        ],
        in_specs=[ANY] + [VMEM] * 9,
        out_specs=[ANY, ANY, VMEM, VMEM],
        scratch_shapes=[
            pltpu.VMEM(x.shape, x.dtype),
            pltpu.VMEM((2, height, wide), x.dtype),
            DMA((2,)),
            DMA((12,)),
            DMA((12,)),
            DMA((72,)),
            DMA((72,)),
        ],
        compiler_params=pltpu.CompilerParams(
            collective_id=2, has_side_effects=True, vmem_limit_bytes=32 * 1024 * 1024
        ),
        cost_estimate=pl.CostEstimate(flops=10**10, bytes_accessed=10**6, transcendentals=0),
    )(x, latents, key_plain, value_up, turned, qlat, query_plain, query_rotary, cosine, sine)


class Fold:
    def __init__(self, part, far, near, mixed, sends, recvs):
        self.part, self.far, self.near, self.mixed = part, far, near, mixed
        ep, tp, right, left, across = ring_places()
        self.tp, self.sides = tp, (right, left)
        self.places = ((ep, right), (ep, left))
        self.size = size = part.shape[1] // 4
        self.at = [pl.ds(c * size, size) for c in range(4)]
        self.hops = []
        self.plain = []
        self.joined = []
        for c in range(4):
            way = c // 2
            other = 1 - way
            self.hops.append(
                remote(part.at[across, self.at[c]], far.at[c], sends, recvs, c, self.places[way])
            )
            self.plain.append(
                remote(
                    part.at[self.sides[other], self.at[c]],
                    near.at[c],
                    sends,
                    recvs,
                    4 + c,
                    self.places[other],
                )
            )
            self.joined.append(
                remote(mixed.at[c], far.at[4 + c], sends, recvs, 8 + c, self.places[way])
            )

    def open(self):
        greet(list(self.places))
        for c in (0, 2, 1, 3):
            self.hops[c].start()
        for c in (2, 0, 3, 1):
            self.plain[c].start()

    def join(self, c):
        own = self.part[self.sides[c // 2], self.at[c], :]
        self.mixed[c] = (own.astype(jnp.float32) + self.far[c].astype(jnp.float32)).astype(
            jnp.bfloat16
        )

    def total(self, c):
        self.joined[c].wait_recv()
        own = self.part[self.tp, self.at[c], :].astype(jnp.float32)
        return own + self.near[c].astype(jnp.float32) + self.far[4 + c].astype(jnp.float32)

    def close(self):
        for copy in self.hops + self.plain + self.joined:
            copy.wait_send()


def fold_scratch(rows, width):
    return [
        pltpu.VMEM((8, rows // 4, width), jnp.bfloat16),
        pltpu.VMEM((4, rows // 4, width), jnp.bfloat16),
        pltpu.VMEM((4, rows // 4, width), jnp.bfloat16),
        DMA((12,)),
        DMA((12,)),
    ]


def finish_kernel(part, gain, rows, out, rows_out, kept, own_sem, far, near, mixed, sends, recvs, row_sends, row_recvs):
    ep, tp, right, left, across = ring_places()
    peers = rows.shape[0]
    swaps = [(partner(ep, r), tp) for r in range(1, peers)]
    barrier = pltpu.get_barrier_semaphore()
    for place in swaps:
        pl.semaphore_signal(barrier, inc=1, device_id=place, device_id_type=MESH)
    fold = Fold(part, far, near, mixed, sends, recvs)
    for place in fold.places:
        pl.semaphore_signal(barrier, inc=1, device_id=place, device_id_type=MESH)
    pl.semaphore_wait(barrier, len(swaps) + 2)
    for c in (0, 2, 1, 3):
        fold.hops[c].start()
    for c in (2, 0, 3, 1):
        fold.plain[c].start()
    moves = [
        remote(rows.at[r], rows_out.at[r], row_sends, row_recvs, r - 1, swaps[r - 1])
        for r in range(1, peers)
    ]
    for copy in moves:
        copy.start()
    take = pltpu.make_async_copy(rows.at[0], kept, own_sem.at[0])
    take.start()
    take.wait()
    put = pltpu.make_async_copy(kept, rows_out.at[0], own_sem.at[0])
    put.start()
    for c in (0, 2):
        fold.hops[c].wait_recv()
        fold.join(c)
    for c in (1, 3):
        fold.hops[c].wait_recv()
    for c in (0, 2):
        fold.joined[c].start()
    for c in (1, 3):
        fold.join(c)
    for c in (0, 2):
        fold.plain[c].wait_recv()
    for c in (1, 3):
        fold.joined[c].start()
        fold.plain[c].wait_recv()
    for c in range(4):
        whole = fold.total(c)
        scale = lax.rsqrt(jnp.mean(whole * whole, axis=-1, keepdims=True) + EPS)
        out[fold.at[c], :] = (whole * scale * gain[...]).astype(jnp.bfloat16)
    fold.close()
    for copy in moves:
        copy.wait()
    put.wait()


def finish(part, gain, rows):
    groups, count, width = part.shape
    peers = rows.shape[0]
    return pl.pallas_call(
        finish_kernel,
        out_shape=[
            jax.ShapeDtypeStruct((count, width), jnp.bfloat16),
            jax.ShapeDtypeStruct(rows.shape, rows.dtype),
        ],
        in_specs=[VMEM, VMEM, ANY],
        out_specs=[VMEM, ANY],
        scratch_shapes=[pltpu.VMEM(rows.shape[1:], rows.dtype), DMA((1,))]
        + fold_scratch(count, width)
        + [DMA((peers - 1,)), DMA((peers - 1,))],
        compiler_params=pltpu.CompilerParams(
            collective_id=3, has_side_effects=True, vmem_limit_bytes=16 * 1024 * 1024
        ),
        cost_estimate=pl.CostEstimate(flops=10**10, bytes_accessed=10**6, transcendentals=0),
    )(part, gain.reshape(1, width), rows)


def attend_kernel(
    heads, qn_ref, qt_ref, kv_ref, part, o_ref, sum_ref, rhs, s_buf, p_buf, peak, acc, *fold_refs
):
    step = pl.program_id(0)
    steps = pl.num_programs(0)
    fold = Fold(part, *fold_refs)

    @pl.when(step == 0)
    def _():
        fold.open()

    @pl.when(step == steps * 5 // 16)
    def _():
        for c in range(4):
            fold.hops[c].wait_recv()
            fold.join(c)

    @pl.when(step == steps * 5 // 16 + 1)
    def _():
        for c in (0, 2, 1, 3):
            fold.joined[c].start()

    pair, wide = kv_ref.shape[0], kv_ref.shape[2]
    size = wide // 2
    subs = size // SUB
    rows = pair * SUB
    queries = qn_ref.shape[1]

    @pl.when(step == 0)
    def _():
        rhs[...] = jnp.zeros_like(rhs)
        for h in range(heads):
            for j in range(subs):
                at = h % 2 * NOPE
                rhs[h, j, at : at + NOPE, :] = qn_ref[h * NOPE : (h + 1) * NOPE, :]
                low = 128 + j * ROPE
                rhs[h, j, low : low + ROPE, :] = qt_ref[h * ROPE : (h + 1) * ROPE, :]
        peak[...] = jnp.full_like(peak, -1e30)
        acc[...] = jnp.zeros_like(acc)

    turned = jnp.concatenate(
        [kv_ref[b, size:, g * 128 : (g + 1) * 128] for b in range(pair) for g in range(wide // 128)],
        axis=0,
    )

    def scores(h):
        half = size // 2
        best = None
        for j in range(subs):
            at = j * SUB % half
            lanes = j * SUB // half * size + h // 2 * 128
            left = jnp.concatenate(
                [kv_ref[b, at : at + SUB, lanes : lanes + 128] for b in range(pair)], axis=0
            )
            left = jnp.concatenate([left, turned], axis=1)
            part = jnp.dot(left, rhs[h, j], preferred_element_type=jnp.float32)
            for b in range(pair):
                s_buf[h % 2, b * size + j * SUB : b * size + (j + 1) * SUB, :] = part[
                    b * SUB : (b + 1) * SUB
                ]
            top = jnp.max(part.reshape(rows // 8, 8, queries), axis=0)
            best = top if best is None else jnp.maximum(best, top)
        return jnp.max(best, axis=0, keepdims=True)

    def finish(h, best):
        old = peak[h : h + 1, :]
        new = jnp.maximum(old, best)
        peak[h : h + 1, :] = new
        shrink = jnp.exp2((old - new) * C)
        base = new * C
        for b in range(pair):
            at = slice(b * size, (b + 1) * size)
            p_buf[h % 2, at, :] = jnp.exp2(s_buf[h % 2, at, :] * C - base).astype(jnp.bfloat16)
        half = size // 2
        at = h * VDIM % half
        lanes = h * VDIM // half * size
        left = jnp.concatenate(
            [
                kv_ref[b, half + at : half + at + VDIM, lanes : lanes + size]
                for b in range(pair)
            ],
            axis=1,
        )
        left = jnp.concatenate([left, jnp.ones((16, left.shape[1]), jnp.bfloat16)], axis=0)
        more = jnp.dot(left, p_buf[h % 2], preferred_element_type=jnp.float32)
        acc[h] = acc[h] * shrink + more

    best = scores(0)
    for h in range(heads):
        later = scores(h + 1) if h + 1 < heads else None
        finish(h, best)
        best = later

    @pl.when(step == steps - 1)
    def _():
        for c in range(4):
            fold.plain[c].wait_recv()
            sum_ref[fold.at[c], :] = fold.total(c).astype(jnp.bfloat16)
        fold.close()
        for h in range(heads):
            o_ref[h * VDIM : (h + 1) * VDIM, :] = (
                acc[h, :VDIM, :] / acc[h, VDIM : VDIM + 1, :]
            ).astype(jnp.bfloat16)


def attend(qn, qt, packed, part, pair=4):
    heads = qn.shape[0] // NOPE
    queries = qn.shape[1]
    blocks, height, wide = packed.shape
    size = wide // 2
    subs = size // SUB
    return pl.pallas_call(
        functools.partial(attend_kernel, heads),
        out_shape=[
            jax.ShapeDtypeStruct((heads * VDIM, queries), jnp.bfloat16),
            jax.ShapeDtypeStruct(part.shape[1:], jnp.bfloat16),
        ],
        grid=(blocks // pair,),
        in_specs=[
            pl.BlockSpec(qn.shape, lambda i: (0, 0)),
            pl.BlockSpec(qt.shape, lambda i: (0, 0)),
            pl.BlockSpec((pair, height, wide), lambda i: (i, 0, 0)),
            VMEM,
        ],
        out_specs=[
            pl.BlockSpec((heads * VDIM, queries), lambda i: (0, 0)),
            pl.BlockSpec(part.shape[1:], lambda i: (0, 0)),
        ],
        scratch_shapes=[
            pltpu.VMEM((heads, subs, 256, queries), jnp.bfloat16),
            pltpu.VMEM((2, pair * size, queries), jnp.float32),
            pltpu.VMEM((2, pair * size, queries), jnp.bfloat16),
            pltpu.VMEM((8, queries), jnp.float32),
            pltpu.VMEM((heads, VDIM + 16, queries), jnp.float32),
        ]
        + fold_scratch(part.shape[1], part.shape[2]),
        compiler_params=pltpu.CompilerParams(
            dimension_semantics=("arbitrary",),
            vmem_limit_bytes=56 * 1024 * 1024,
            collective_id=4,
            has_side_effects=True,
        ),
        cost_estimate=pl.CostEstimate(
            flops=2 * heads * queries * blocks * size * (256 + VDIM),
            bytes_accessed=blocks * height * wide * 2,
            transcendentals=heads * queries * blocks * size,
        ),
    )(qn, qt, packed, part)


def norm_rows(values, gain):
    values = values.astype(jnp.float32)
    scale = lax.rsqrt(jnp.mean(values * values, axis=-1, keepdims=True) + EPS)
    return values * scale * gain


def turn_tables(positions, width):
    half = width // 2
    freqs = THETA ** (-2.0 * jnp.arange(half, dtype=jnp.float32) / width)
    angles = positions.astype(jnp.float32)[:, None] * freqs[None, :]
    return (jnp.cos(angles), jnp.sin(angles))


def rotate(values, cosine, sine):
    half = values.shape[-1] // 2
    first = values[..., :half]
    second = values[..., half:]
    return jnp.concatenate(
        [first * cosine - second * sine, second * cosine + first * sine], axis=-1
    )


def on_device(
    mixer_input,
    expert_input,
    mixer_gain,
    query_down,
    latent_down,
    rotary_down,
    query_gain,
    latent_gain,
    query_plain,
    query_rotary,
    key_plain,
    value_up,
    output_proj,
    mixed_gain,
    expert_norm,
    route_ids,
    route_weight,
    gate_proj,
    up_proj,
    down_proj,
    expert_gain,
):
    tok_rows = mixer_input.shape[0]
    groups = lax.axis_size("tp")
    group_base = lax.axis_index("ep") * groups * tok_rows
    offset = group_base + lax.axis_index("tp") * tok_rows
    hidden = norm_rows(mixer_input, mixer_gain).astype(jnp.bfloat16)
    query_lat = norm_rows(
        jnp.dot(hidden, query_down, preferred_element_type=jnp.float32), query_gain
    ).astype(jnp.bfloat16)
    key_lat = norm_rows(
        jnp.dot(hidden, latent_down, preferred_element_type=jnp.float32), latent_gain
    ).astype(jnp.bfloat16)
    cosine, sine = turn_tables(offset + jnp.arange(tok_rows, dtype=jnp.int32), ROPE)
    key_turn = rotate(
        jnp.dot(hidden, rotary_down, preferred_element_type=jnp.float32), cosine, sine
    ).astype(jnp.bfloat16)
    expert_hidden = norm_rows(expert_input, expert_norm).astype(jnp.bfloat16)
    experts = lax.axis_size("ep")
    topk = route_ids.shape[1]
    capacity = 5 * tok_rows * topk // (4 * experts)
    slots = experts * capacity
    flat_ids = route_ids.reshape(-1)
    onehot = (flat_ids[:, None] == jnp.arange(experts, dtype=jnp.int32)[None, :]).astype(jnp.int32)
    order = jnp.sum((jnp.cumsum(onehot, axis=0) - onehot) * onehot, axis=1)
    target = (flat_ids ^ lax.axis_index("ep")) * capacity + order
    dispatch = jnp.any(
        target.reshape(tok_rows, topk)[None, :, :]
        == jnp.arange(slots, dtype=jnp.int32)[:, None, None],
        axis=2,
    ).astype(jnp.bfloat16)
    outgoing = (
        jnp.dot(dispatch, expert_hidden, preferred_element_type=jnp.float32)
        .astype(jnp.bfloat16)
        .reshape(experts, capacity, expert_hidden.shape[1] // 128, 128)
    )
    wide_turn = jnp.pad(key_turn, ((0, 0), (0, 128 - ROPE)))
    latents, turned, qlat, received = exchange((key_lat, wide_turn, query_lat), outgoing)
    count = groups * tok_rows
    latents = latents.reshape(count, latents.shape[2])
    qlat = qlat.reshape(count, qlat.shape[2])
    turned = turned[:, :, :ROPE].reshape(2, 4, 4, 16, ROPE).transpose(0, 3, 2, 1, 4)
    turned = turned.reshape(2, 16, 4 * 4 * ROPE)
    all_cos, all_sin = turn_tables(group_base + jnp.arange(count, dtype=jnp.int32), ROPE)
    width = expert_hidden.shape[1]
    piece, packed, qn, qt = gather(
        received.reshape(slots, width),
        latents,
        key_plain,
        value_up,
        turned,
        qlat,
        query_plain,
        query_rotary,
        all_cos.T,
        all_sin.T,
    )
    piece = piece.reshape(groups * slots, width)
    packed = packed.reshape(-1, *packed.shape[2:])
    gate_w = gate_proj[0]
    up_w = up_proj[0]
    down_w = down_proj[0]
    gate = jnp.minimum(jnp.dot(piece, gate_w, preferred_element_type=jnp.float32), CLAMP)
    up = jnp.clip(jnp.dot(piece, up_w, preferred_element_type=jnp.float32), -CLAMP, CLAMP)
    acts = ((up + 1.0) * gate * jax.nn.sigmoid(ALPHA * gate)).astype(jnp.bfloat16)
    part = jnp.dot(acts, down_w, preferred_element_type=jnp.float32).astype(jnp.bfloat16)
    attended, sums = attend(qn, qt, packed, part.reshape(groups, slots, width))
    mixed = lax.dot_general(
        attended, output_proj, (((0,), (0,)), ((), ())), preferred_element_type=jnp.float32
    ).astype(jnp.bfloat16)
    mixer_out, back_rows = finish(
        mixed.reshape(groups, tok_rows, width),
        mixed_gain,
        sums.reshape(experts, capacity, width // 128, 128),
    )
    back_rows = back_rows.reshape(slots, width // 128, 128)
    picked = back_rows[target].astype(jnp.float32).reshape(tok_rows, topk, width // 128, 128)
    combined = jnp.sum(picked * route_weight[:, :, None, None], axis=1).reshape(tok_rows, width)
    expert_out = norm_rows(combined, expert_gain).astype(jnp.bfloat16)
    return (mixer_out, expert_out)


def solution(mesh):
    in_specs = (
        P(("ep", "tp"), None),
        P(("ep", "tp"), None),
        P(),
        P(),
        P(),
        P(),
        P(),
        P(),
        P(None, "tp"),
        P(None, "tp"),
        P(None, "tp"),
        P(None, "tp"),
        P("tp", None),
        P(),
        P(),
        P(("ep", "tp"), None),
        P(("ep", "tp"), None),
        P("ep", None, "tp"),
        P("ep", None, "tp"),
        P("ep", "tp", None),
        P(),
    )
    out_specs = (P(("ep", "tp"), None), P(("ep", "tp"), None))
    return jax.shard_map(
        on_device, mesh=mesh, in_specs=in_specs, out_specs=out_specs, check_vma=False
    )
```

```python
import functools

import jax
import jax.numpy as jnp
from jax import lax
from jax.experimental import pallas as pl
from jax.experimental.pallas import tpu as pltpu
from jax.sharding import PartitionSpec as P

NOPE = 64
ROPE = 32
VDIM = 64


EPS = 1e-06
CLAMP = 7.0
ALPHA = 1.702
THETA = 10000.0
FLOOR = -1e30
LOG2E = 1.4426950408889634
C = (NOPE + ROPE) ** (-0.5) * LOG2E
SUB = 64

MESH = pl.DeviceIdType.MESH
ANY = pl.BlockSpec(memory_space=pl.ANY)
HBM = pl.BlockSpec(memory_space=pltpu.HBM)
VMEM = pl.BlockSpec(memory_space=pltpu.VMEM)
DMA = pltpu.SemaphoreType.DMA


def ring_places():
    ep, tp, n = lax.axis_index("ep"), lax.axis_index("tp"), lax.axis_size("tp")
    right = lax.rem(tp + 1, n)
    left = lax.rem(tp + n - 1, n)
    across = lax.rem(tp + 2, n)
    return ep, tp, right, left, across


def partner(ep, r):
    for bit in range(r.bit_length()):
        if r >> bit & 1:
            ep = ep + (1 - 2 * lax.rem(ep // (1 << bit), 2)) * (1 << bit)
    return ep


def greet(places):
    barrier = pltpu.get_barrier_semaphore()
    for place in places:
        pl.semaphore_signal(barrier, inc=1, device_id=place, device_id_type=MESH)
    pl.semaphore_wait(barrier, len(places))


def remote(src, dst, sends, recvs, k, place):
    return pltpu.make_async_remote_copy(
        src_ref=src,
        dst_ref=dst,
        send_sem=sends.at[k],
        recv_sem=recvs.at[k],
        device_id=place,
        device_id_type=MESH,
    )


def exchange_kernel(latent_count, *refs):
    lats, rows = refs[:latent_count], refs[latent_count]
    outs, rows_out = refs[latent_count + 1 : 2 * latent_count + 1], refs[2 * latent_count + 1]
    kept, kept_rows = refs[2 * latent_count + 2 : 3 * latent_count + 2], refs[3 * latent_count + 2]
    own_sem, sends, recvs, row_sends, row_recvs = refs[3 * latent_count + 3 :]
    ep, tp, right, left, across = ring_places()
    peers = rows.shape[0]
    swaps = [(partner(ep, r), tp) for r in range(1, peers)]
    to_right, to_left = (ep, right), (ep, left)
    greet(swaps + [to_right, to_left])
    own = [
        pltpu.make_async_copy(src, dst, own_sem.at[k])
        for k, (src, dst) in enumerate(
            [(a, b) for a, b in zip(lats, kept)] + [(rows.at[0], kept_rows)]
        )
    ]
    first, second, waits = [], [], []
    for k, (lat, out) in enumerate(zip(lats, outs)):
        half = lat.shape[0] // 2
        for part, place in ((0, to_right), (1, to_left), (1, to_right), (0, to_left)):
            way = 0 if place is to_right else 1
            at = pl.ds(part * half, half)
            first.append(
                remote(
                    lat.at[at], out.at[tp, at], sends, recvs, 6 * k + 2 * way + part, place
                )
            )
        for way, place, origin in ((0, to_right, left), (1, to_left, right)):
            at = pl.ds(way * half, half)
            second.append(
                remote(
                    out.at[origin, at], out.at[origin, at], sends, recvs, 6 * k + 4 + way, place
                )
            )
    moves = [
        remote(rows.at[r], rows_out.at[r], row_sends, row_recvs, r - 1, swaps[r - 1])
        for r in range(1, peers)
    ]
    for copy in first:
        copy.start()
    for copy in moves:
        copy.start()
    for copy in own:
        copy.start()
    for copy in own:
        copy.wait()
    back = [
        pltpu.make_async_copy(src, dst, own_sem.at[k])
        for k, (src, dst) in enumerate(
            [(a, b.at[tp]) for a, b in zip(kept, outs)] + [(kept_rows, rows_out.at[0])]
        )
    ]
    for copy in back:
        copy.start()
    for k in range(latent_count):
        first[4 * k].wait_recv()
        second[2 * k].start()
        first[4 * k + 1].wait_recv()
        second[2 * k + 1].start()
    for k in range(latent_count):
        first[4 * k + 2].wait_recv()
        first[4 * k + 3].wait_recv()
    for copy in second:
        copy.wait_recv()
    for copy in moves:
        copy.wait_recv()
    for copy in first + second + moves:
        copy.wait_send()
    for copy in back:
        copy.wait()


def exchange(lats, rows):
    groups = lax.axis_size("tp")
    count = len(lats)
    peers = rows.shape[0]
    return pl.pallas_call(
        functools.partial(exchange_kernel, count),
        out_shape=[jax.ShapeDtypeStruct((groups, *a.shape), a.dtype) for a in lats]
        + [jax.ShapeDtypeStruct(rows.shape, rows.dtype)],
        in_specs=[ANY] * (count + 1),
        out_specs=[HBM] * (count + 1),
        scratch_shapes=[pltpu.VMEM(a.shape, a.dtype) for a in lats]
        + [
            pltpu.VMEM(rows.shape[1:], rows.dtype),
            DMA((count + 1,)),
            DMA((6 * count,)),
            DMA((6 * count,)),
            DMA((peers - 1,)),
            DMA((peers - 1,)),
        ],
        compiler_params=pltpu.CompilerParams(
            collective_id=1, has_side_effects=True, vmem_limit_bytes=8 * 1024 * 1024
        ),
        cost_estimate=pl.CostEstimate(flops=10**10, bytes_accessed=10**6, transcendentals=0),
    )(*lats, rows)


KV_ORDER = (
    [(f, 0, 0, p) for p in range(2) for f in range(2)]
    + [(f, a, 0, p) for p in range(2) for f in range(2) for a in (3, 1)]
    + [(f, 0, b, p) for p in range(2) for f in range(2) for b in (3, 1)]
    + [(f, 2, 0, p) for p in range(2) for f in range(2)]
    + [(f, 3, b, p) for p in range(2) for f in range(2) for b in (3, 1)]
    + [(f, 1, b, p) for p in range(2) for f in range(2) for b in (3, 1)]
    + [(f, 0, 2, p) for p in range(2) for f in range(2)]
    + [(f, 2, b, p) for p in range(2) for f in range(2) for b in (3, 1)]
    + [(f, a, 2, p) for a in (3, 1, 2) for p in range(2) for f in range(2)]
)
KV_SLOT = {key: k for k, key in enumerate(KV_ORDER)}

OWN, LEFT, RIGHT, FAR = range(4)
ROW_ORDER = (
    [(OWN, 0), (OWN, 1), (LEFT, 0), (RIGHT, 2), (LEFT, 1), (RIGHT, 3), (OWN, 2), (FAR, 0)]
    + [(FAR, 2), (FAR, 1), (FAR, 3), (RIGHT, 0), (LEFT, 2), (RIGHT, 1), (LEFT, 3), (OWN, 3)]
)
ROW_SLOT = {key: k for k, key in enumerate(ROW_ORDER)}
BACK = (3, 1)


class Spread:
    def __init__(self, held, sends, recvs):
        ep, tp = lax.axis_index("ep"), lax.axis_index("tp")
        side = 4
        core = lax.rem(ep, 2)
        y = lax.rem(ep // 2, side)
        z = ep // (2 * side)
        self.held, self.sends, self.recvs = held, sends, recvs
        self.mate = (ep + 1 - 2 * core, tp)
        cut = held.shape[1] // 32 * 16
        self.parts = (pl.ds(0, cut), pl.ds(cut, held.shape[1] - cut))

        def index(dz, dy):
            return ((lax.rem(z + dz, side) * side + lax.rem(y + dy, side)) * 2 + core, tp)

        around = [(index(0, 1), index(0, 3)), (index(1, 0), index(3, 0))]
        self.places = [around, around[::-1]]
        self.neighbours = [place for pair in around for place in pair] + [self.mate]

    def copy(self, f, here, there, place, k, part=None):
        src = self.held.at[KV_SLOT[(f, *here)]]
        dst = self.held.at[KV_SLOT[(f, *there)]]
        if part is not None:
            src, dst = src.at[self.parts[part]], dst.at[self.parts[part]]
        return remote(src, dst, self.sends, self.recvs, 36 * f + k, place)

    def first(self, f, way):
        return self.copy(f, (0, 0, 0), (BACK[way], 0, 0), self.places[f][0][way], way)

    def first_on(self, f, way):
        return self.copy(
            f, (BACK[way], 0, 0), (2, 0, 0), self.places[f][0][way], 2 + way, part=way
        )

    def second(self, f, a, way):
        return self.copy(f, (a, 0, 0), (a, BACK[way], 0), self.places[f][1][way], 4 + 4 * a + way)

    def second_on(self, f, a, way):
        return self.copy(
            f, (a, BACK[way], 0), (a, 2, 0), self.places[f][1][way], 6 + 4 * a + way, part=way
        )

    def share(self, f, a, b):
        return self.copy(f, (a, b, 0), (a, b, 1), self.mate, 20 + 4 * a + b)

    def start(self):
        for f in range(2):
            for way in range(2):
                self.first(f, way).start()
        for f in range(2):
            self.share(f, 0, 0).start()
            for way in range(2):
                self.second(f, 0, way).start()

    def got_first(self):
        for f in range(2):
            for way in range(2):
                self.first(f, way).wait_recv()
                self.first_on(f, way).start()
                a = BACK[way]
                for there in range(2):
                    self.second(f, a, there).start()
                self.share(f, a, 0).start()

    def got_second(self, a):
        for f in range(2):
            for way in range(2):
                self.second(f, a, way).wait_recv()
                self.second_on(f, a, way).start()
                self.share(f, a, BACK[way]).start()

    def got_far_first(self):
        for f in range(2):
            for way in range(2):
                self.first_on(f, way).wait_recv()
            for there in range(2):
                self.second(f, 2, there).start()
            self.share(f, 2, 0).start()

    def got_far_second(self, a):
        for f in range(2):
            for way in range(2):
                self.second_on(f, a, way).wait_recv()
            self.share(f, a, 2).start()

    def got_shares(self, *spots):
        for f in range(2):
            for a, b in spots:
                self.share(f, a, b).wait_recv()

    def close(self):
        for f in range(2):
            for a in range(4):
                for b in range(4):
                    self.share(f, a, b).wait_send()
            for way in range(2):
                self.first(f, way).wait_send()
                self.first_on(f, way).wait_send()
                for a in range(4):
                    self.second(f, a, way).wait_send()
                    self.second_on(f, a, way).wait_send()


class Ring:
    def __init__(self, x, rows, sends, recvs):
        ep, tp, right, left, across = ring_places()
        self.places = ((ep, right), (ep, left))
        size = rows.shape[1]
        self.news, self.passed, self.own = {}, [], []
        for c in range(4):
            chunk = x.at[pl.ds(c * size, size)]
            for way in range(2):
                origin = (LEFT, RIGHT)[way]
                self.news[c, way] = remote(
                    chunk, rows.at[ROW_SLOT[origin, c]], sends, recvs, 4 * way + c, self.places[way]
                )
            way = c // 2
            origin = (LEFT, RIGHT)[way]
            self.passed.append(
                remote(
                    rows.at[ROW_SLOT[origin, c]],
                    rows.at[ROW_SLOT[FAR, c]],
                    sends,
                    recvs,
                    8 + c,
                    self.places[way],
                )
            )

    def start(self):
        for key in ((0, 0), (2, 1), (1, 0), (3, 1)):
            self.news[key].start()

    def relay(self, c):
        self.news[c, 0].wait_recv()
        self.passed[c].start()
        self.news[2 + c, 0].start()
        self.news[2 + c, 1].wait_recv()
        self.passed[2 + c].start()
        self.news[c, 1].start()

    def arrived(self, whose, c):
        if whose == FAR:
            self.passed[c].wait_recv()
        elif whose in (LEFT, RIGHT) and c // 2 != whose - LEFT:
            self.news[c, whose - LEFT].wait_recv()

    def close(self):
        for copy in self.passed + list(self.news.values()):
            copy.wait_send()


class Fold:
    def __init__(self, part, far, near, mixed, sends, recvs):
        self.part, self.far, self.near, self.mixed = part, far, near, mixed
        ep, tp, right, left, across = ring_places()
        self.places = ((ep, right), (ep, left))
        self.hops, self.plain, self.joined = [], [], []
        for c in range(4):
            way = c // 2
            other = 1 - way
            self.hops.append(remote(part(FAR, c), far.at[c], sends, recvs, c, self.places[way]))
            self.plain.append(
                remote(
                    part((RIGHT, LEFT)[other], c), near.at[c], sends, recvs, 4 + c, self.places[other]
                )
            )
            self.joined.append(
                remote(mixed.at[c], far.at[4 + c], sends, recvs, 8 + c, self.places[way])
            )

    def join(self, c):
        own = self.part((RIGHT, LEFT)[c // 2], c)[...]
        self.mixed[c] = (own.astype(jnp.float32) + self.far[c].astype(jnp.float32)).astype(
            jnp.bfloat16
        )

    def total(self, c):
        self.joined[c].wait_recv()
        own = self.part(OWN, c)[...].astype(jnp.float32)
        return own + self.near[c].astype(jnp.float32) + self.far[4 + c].astype(jnp.float32)

    def close(self):
        for copy in self.hops + self.plain + self.joined:
            copy.wait_send()


def fold_scratch(rows, width):
    return [
        pltpu.VMEM((8, rows // 4, width), jnp.bfloat16),
        pltpu.VMEM((4, rows // 4, width), jnp.bfloat16),
        pltpu.VMEM((4, rows // 4, width), jnp.bfloat16),
        DMA((12,)),
        DMA((12,)),
    ]


def finish_kernel(part, gain, rows, out, rows_out, kept, own_sem, far, near, mixed, sends, recvs, row_sends, row_recvs):
    ep, tp, right, left, across = ring_places()
    peers = rows.shape[0]
    swaps = [(partner(ep, r), tp) for r in range(1, peers)]
    barrier = pltpu.get_barrier_semaphore()
    for place in swaps:
        pl.semaphore_signal(barrier, inc=1, device_id=place, device_id_type=MESH)
    size = part.shape[1] // 4

    def piece(whose, c):
        return part.at[(tp, left, right, across)[whose], pl.ds(c * size, size)]

    fold = Fold(piece, far, near, mixed, sends, recvs)
    for place in fold.places:
        pl.semaphore_signal(barrier, inc=1, device_id=place, device_id_type=MESH)
    pl.semaphore_wait(barrier, len(swaps) + 2)
    for c in (0, 2, 1, 3):
        fold.hops[c].start()
    for c in (2, 0, 3, 1):
        fold.plain[c].start()
    moves = [
        remote(rows.at[r], rows_out.at[r], row_sends, row_recvs, r - 1, swaps[r - 1])
        for r in range(1, peers)
    ]
    for copy in moves:
        copy.start()
    take = pltpu.make_async_copy(rows.at[0], kept, own_sem.at[0])
    take.start()
    take.wait()
    put = pltpu.make_async_copy(kept, rows_out.at[0], own_sem.at[0])
    put.start()
    for c in (0, 2):
        fold.hops[c].wait_recv()
        fold.join(c)
    for c in (1, 3):
        fold.hops[c].wait_recv()
    for c in (0, 2):
        fold.joined[c].start()
    for c in (1, 3):
        fold.join(c)
    for c in (0, 2):
        fold.plain[c].wait_recv()
    for c in (1, 3):
        fold.joined[c].start()
        fold.plain[c].wait_recv()
    for c in range(4):
        whole = fold.total(c)
        scale = lax.rsqrt(jnp.mean(whole * whole, axis=-1, keepdims=True) + EPS)
        out[c * size : (c + 1) * size, :] = (whole * scale * gain[...]).astype(jnp.bfloat16)
    fold.close()
    for copy in moves:
        copy.wait()
    put.wait()


def finish(part, gain, rows):
    groups, count, width = part.shape
    peers = rows.shape[0]
    return pl.pallas_call(
        finish_kernel,
        out_shape=[
            jax.ShapeDtypeStruct((count, width), jnp.bfloat16),
            jax.ShapeDtypeStruct(rows.shape, rows.dtype),
        ],
        in_specs=[VMEM, VMEM, ANY],
        out_specs=[VMEM, ANY],
        scratch_shapes=[pltpu.VMEM(rows.shape[1:], rows.dtype), DMA((1,))]
        + fold_scratch(count, width)
        + [DMA((peers - 1,)), DMA((peers - 1,))],
        compiler_params=pltpu.CompilerParams(
            collective_id=3, has_side_effects=True, vmem_limit_bytes=16 * 1024 * 1024
        ),
        cost_estimate=pl.CostEstimate(flops=10**10, bytes_accessed=10**6, transcendentals=0),
    )(part, gain.reshape(1, width), rows)


def core_kernel(
    x,
    latents_in,
    qlat_in,
    turned,
    key_plain_in,
    value_up_in,
    query_plain_in,
    query_rotary_in,
    gate_in,
    up_in,
    down_in,
    cosine,
    sine,
    o_ref,
    sum_ref,
    rhs,
    s_buf,
    p_buf,
    peak,
    acc,
    held,
    rows,
    part,
    latents,
    qlat,
    key_plain,
    value_up,
    query_plain,
    query_rotary,
    gate_w,
    up_w,
    down_w,
    load_sem,
    row_sends,
    row_recvs,
    kv_sends,
    kv_recvs,
    *fold_refs,
):
    step = pl.program_id(0)
    heads = acc.shape[0]
    pair = 4
    wide = held.shape[2]
    size = wide // 2
    subs = size // SUB
    count = pair * SUB
    queries = o_ref.shape[1]
    chunk_rows = rows.shape[1]
    spread = Spread(held, kv_sends, kv_recvs)
    ring = Ring(x, rows, row_sends, row_recvs)
    fold = Fold(lambda whose, c: part.at[ROW_SLOT[whose, c]], *fold_refs)
    loads = [
        pltpu.make_async_copy(src, dst, load_sem.at[k])
        for k, (src, dst) in enumerate(
            [
                (latents_in, latents),
                (key_plain_in, key_plain),
                (value_up_in, value_up),
                (qlat_in, qlat),
                (query_plain_in, query_plain),
                (query_rotary_in, query_rotary),
                (gate_in, gate_w),
                (up_in, up_w),
                (down_in, down_w),
            ]
        )
    ]
    takes = [
        pltpu.make_async_copy(
            x.at[pl.ds(c * chunk_rows, chunk_rows)], rows.at[ROW_SLOT[OWN, c]], load_sem.at[9 + c]
        )
        for c in range(4)
    ]

    @pl.when(step == 0)
    def _():
        barrier = pltpu.get_barrier_semaphore()
        places = list(ring.places) + spread.neighbours
        for place in places:
            pl.semaphore_signal(barrier, inc=1, device_id=place, device_id_type=MESH)
        for copy in loads[:3] + takes + loads[3:]:
            copy.start()
        pl.semaphore_wait(barrier, len(places))
        ring.start()
        for copy in loads[:3]:
            copy.wait()
        keys = jnp.dot(latents[...], key_plain[...], preferred_element_type=jnp.float32)
        values = jnp.dot(latents[...], value_up[...], preferred_element_type=jnp.float32).T
        keys, values = keys.astype(jnp.bfloat16), values.astype(jnp.bfloat16)
        half = size // 2
        for f in range(2):
            own = KV_SLOT[f, 0, 0, 0]
            held[own, :half, :size] = keys[size * f : size * f + half]
            held[own, :half, size:] = keys[size * f + half : size * f + size]
            held[own, half:size, :size] = values[:half, size * f : size * f + size]
            held[own, half:size, size:] = values[half:, size * f : size * f + size]
            held[own, size:, :] = turned[f]
        rhs[...] = jnp.zeros_like(rhs)
        peak[...] = jnp.full_like(peak, FLOOR)
        acc[...] = jnp.zeros_like(acc)
        spread.start()
        for copy in loads[3:6]:
            copy.wait()
        plain = jnp.dot(qlat[...], query_plain[...], preferred_element_type=jnp.float32)
        plain = plain.T.astype(jnp.bfloat16)
        rotated = jnp.dot(qlat[...], query_rotary[...], preferred_element_type=jnp.float32).T
        quarter = ROPE // 2
        for h in range(heads):
            a = rotated[h * ROPE : h * ROPE + quarter]
            b = rotated[h * ROPE + quarter : h * ROPE + ROPE]
            first = (a * cosine[...] - b * sine[...]).astype(jnp.bfloat16)
            second = (b * cosine[...] + a * sine[...]).astype(jnp.bfloat16)
            at = h % 2 * NOPE
            for j in range(subs):
                rhs[h, j, at : at + NOPE, :] = plain[h * NOPE : (h + 1) * NOPE]
                low = 128 + j * ROPE
                rhs[h, j, low : low + quarter, :] = first
                rhs[h, j, low + quarter : low + ROPE, :] = second
        for copy in takes + loads[6:]:
            copy.wait()
        spread.got_shares((0, 0))

    plan = {
        1: [lambda: spread.got_first()],
        2: [lambda: ring.relay(0), lambda: spread.got_shares((3, 0), (1, 0))],
        3: [lambda: spread.got_second(0)],
        4: [
            lambda: ring.relay(1),
            lambda: spread.got_shares((0, 3), (0, 1)),
            lambda: spread.got_far_first(),
        ],
        5: [lambda: spread.got_shares((2, 0))],
        6: [lambda: spread.got_second(3)],
        7: [lambda: spread.got_shares((3, 3), (3, 1)), lambda: spread.got_second(1)],
        8: [lambda: fold.hops[0].start()],
        9: [
            lambda: fold.hops[2].start(),
            lambda: spread.got_shares((1, 3), (1, 1)),
            lambda: spread.got_far_second(0),
            lambda: spread.got_second(2),
        ],
        10: [lambda: fold.hops[1].start(), lambda: spread.got_shares((0, 2))]
        + [fold.plain[c].start for c in (2, 0, 3, 1)],
        11: [lambda: fold.hops[3].start(), lambda: spread.got_far_second(3)],
        12: [
            lambda: spread.got_shares((2, 3), (2, 1)),
            lambda: spread.got_far_second(1),
            lambda: fold.hops[0].wait_recv(),
            lambda: fold.join(0),
        ],
        13: [
            lambda: spread.got_shares((3, 2)),
            lambda: fold.joined[0].start(),
            lambda: spread.got_far_second(2),
            lambda: fold.hops[2].wait_recv(),
            lambda: fold.join(2),
        ],
        14: [
            lambda: spread.got_shares((1, 2)),
            lambda: fold.joined[2].start(),
            lambda: fold.hops[1].wait_recv(),
            lambda: fold.join(1),
        ],
        15: [
            lambda: spread.got_shares((2, 2)),
            lambda: fold.joined[1].start(),
            lambda: fold.hops[3].wait_recv(),
            lambda: fold.join(3),
        ],
    }
    for k, actions in plan.items():

        @pl.when(step == k)
        def _(k=k, actions=actions):
            for action in actions:
                action()
            ring.arrived(*ROW_ORDER[k])

    gate = jnp.minimum(
        jnp.dot(rows[step], gate_w[...], preferred_element_type=jnp.float32), CLAMP
    )
    up = jnp.clip(
        jnp.dot(rows[step], up_w[...], preferred_element_type=jnp.float32), -CLAMP, CLAMP
    )
    acts = ((up + 1.0) * gate * jax.nn.sigmoid(ALPHA * gate)).astype(jnp.bfloat16)
    part[step] = jnp.dot(acts, down_w[...], preferred_element_type=jnp.float32).astype(
        jnp.bfloat16
    )

    kv_ref = held.at[pl.ds(pair * step, pair)]
    turns = jnp.concatenate(
        [kv_ref[b, size:, g * 128 : (g + 1) * 128] for b in range(pair) for g in range(wide // 128)],
        axis=0,
    )

    def scores(h):
        half = size // 2
        best = None
        for j in range(subs):
            at = j * SUB % half
            lanes = j * SUB // half * size + h // 2 * 128
            left = jnp.concatenate(
                [kv_ref[b, at : at + SUB, lanes : lanes + 128] for b in range(pair)], axis=0
            )
            left = jnp.concatenate([left, turns], axis=1)
            block = jnp.dot(left, rhs[h, j], preferred_element_type=jnp.float32)
            for b in range(pair):
                s_buf[h % 2, b * size + j * SUB : b * size + (j + 1) * SUB, :] = block[
                    b * SUB : (b + 1) * SUB
                ]
            top = jnp.max(block.reshape(count // 8, 8, queries), axis=0)
            best = top if best is None else jnp.maximum(best, top)
        return jnp.max(best, axis=0, keepdims=True)

    def finish(h, best):
        old = peak[h : h + 1, :]
        new = jnp.maximum(old, best)
        peak[h : h + 1, :] = new
        shrink = jnp.exp2((old - new) * C)
        base = new * C
        for b in range(pair):
            at = slice(b * size, (b + 1) * size)
            p_buf[h % 2, at, :] = jnp.exp2(s_buf[h % 2, at, :] * C - base).astype(jnp.bfloat16)
        half = size // 2
        at = h * VDIM % half
        lanes = h * VDIM // half * size
        left = jnp.concatenate(
            [
                kv_ref[b, half + at : half + at + VDIM, lanes : lanes + size]
                for b in range(pair)
            ],
            axis=1,
        )
        left = jnp.concatenate([left, jnp.ones((16, left.shape[1]), jnp.bfloat16)], axis=0)
        more = jnp.dot(left, p_buf[h % 2], preferred_element_type=jnp.float32)
        acc[h] = acc[h] * shrink + more

    best = scores(0)
    for h in range(heads):
        later = scores(h + 1) if h + 1 < heads else None
        finish(h, best)
        best = later

    @pl.when(step == pl.num_programs(0) - 1)
    def _():
        fold.joined[3].start()
        for h in range(heads):
            o_ref[h * VDIM : (h + 1) * VDIM, :] = (
                acc[h, :VDIM, :] / acc[h, VDIM : VDIM + 1, :]
            ).astype(jnp.bfloat16)
        for c in range(4):
            fold.plain[c].wait_recv()
            sum_ref[c * chunk_rows : (c + 1) * chunk_rows, :] = fold.total(c).astype(jnp.bfloat16)
        fold.close()
        ring.close()
        spread.close()


def core(x, latents, qlat, turned, mats, cosine, sine):
    key_plain, value_up, query_plain, query_rotary, gate_w, up_w, down_w = mats
    heads = query_plain.shape[1] // NOPE
    queries = latents.shape[0]
    size = key_plain.shape[1]
    wide = turned.shape[2]
    height = size + turned.shape[1]
    slots, width = x.shape
    subs = size // SUB
    bf16 = jnp.bfloat16
    return pl.pallas_call(
        core_kernel,
        out_shape=[
            jax.ShapeDtypeStruct((heads * VDIM, queries), bf16),
            jax.ShapeDtypeStruct((slots, width), bf16),
        ],
        grid=(16,),
        in_specs=[HBM] * 3 + [VMEM] + [HBM] * 7 + [VMEM] * 2,
        out_specs=[VMEM, VMEM],
        scratch_shapes=[
            pltpu.VMEM((heads, subs, 256, queries), bf16),
            pltpu.VMEM((2, 4 * size, queries), jnp.float32),
            pltpu.VMEM((2, 4 * size, queries), bf16),
            pltpu.VMEM((8, queries), jnp.float32),
            pltpu.VMEM((heads, VDIM + 16, queries), jnp.float32),
            pltpu.VMEM((64, height, wide), bf16),
            pltpu.VMEM((16, slots // 4, width), bf16),
            pltpu.VMEM((16, slots // 4, width), bf16),
            pltpu.VMEM(latents.shape, bf16),
            pltpu.VMEM(qlat.shape, bf16),
        ]
        + [pltpu.VMEM(a.shape, bf16) for a in mats]
        + [DMA((13,)), DMA((12,)), DMA((12,)), DMA((72,)), DMA((72,))]
        + fold_scratch(slots, width),
        compiler_params=pltpu.CompilerParams(
            dimension_semantics=("arbitrary",),
            vmem_limit_bytes=63 * 1024 * 1024,
            collective_id=4,
            has_side_effects=True,
        ),
        cost_estimate=pl.CostEstimate(flops=10**11, bytes_accessed=10**7, transcendentals=10**7),
    )(x, latents, qlat, turned, *mats, cosine, sine)


def norm_rows(values, gain):
    values = values.astype(jnp.float32)
    scale = lax.rsqrt(jnp.mean(values * values, axis=-1, keepdims=True) + EPS)
    return values * scale * gain


def turn_tables(positions, width):
    half = width // 2
    freqs = THETA ** (-2.0 * jnp.arange(half, dtype=jnp.float32) / width)
    angles = positions.astype(jnp.float32)[:, None] * freqs[None, :]
    return (jnp.cos(angles), jnp.sin(angles))


def rotate(values, cosine, sine):
    half = values.shape[-1] // 2
    first = values[..., :half]
    second = values[..., half:]
    return jnp.concatenate(
        [first * cosine - second * sine, second * cosine + first * sine], axis=-1
    )


def on_device(
    mixer_input,
    expert_input,
    mixer_gain,
    query_down,
    latent_down,
    rotary_down,
    query_gain,
    latent_gain,
    query_plain,
    query_rotary,
    key_plain,
    value_up,
    output_proj,
    mixed_gain,
    expert_norm,
    route_ids,
    route_weight,
    gate_proj,
    up_proj,
    down_proj,
    expert_gain,
):
    tok_rows = mixer_input.shape[0]
    groups = lax.axis_size("tp")
    group_base = lax.axis_index("ep") * groups * tok_rows
    offset = group_base + lax.axis_index("tp") * tok_rows
    hidden = norm_rows(mixer_input, mixer_gain).astype(jnp.bfloat16)
    query_lat = norm_rows(
        jnp.dot(hidden, query_down, preferred_element_type=jnp.float32), query_gain
    ).astype(jnp.bfloat16)
    key_lat = norm_rows(
        jnp.dot(hidden, latent_down, preferred_element_type=jnp.float32), latent_gain
    ).astype(jnp.bfloat16)
    cosine, sine = turn_tables(offset + jnp.arange(tok_rows, dtype=jnp.int32), ROPE)
    key_turn = rotate(
        jnp.dot(hidden, rotary_down, preferred_element_type=jnp.float32), cosine, sine
    ).astype(jnp.bfloat16)
    expert_hidden = norm_rows(expert_input, expert_norm).astype(jnp.bfloat16)
    experts = lax.axis_size("ep")
    topk = route_ids.shape[1]
    capacity = 5 * tok_rows * topk // (4 * experts)
    slots = experts * capacity
    flat_ids = route_ids.reshape(-1)
    onehot = (flat_ids[:, None] == jnp.arange(experts, dtype=jnp.int32)[None, :]).astype(jnp.int32)
    order = jnp.sum((jnp.cumsum(onehot, axis=0) - onehot) * onehot, axis=1)
    target = (flat_ids ^ lax.axis_index("ep")) * capacity + order
    dispatch = jnp.any(
        target.reshape(tok_rows, topk)[None, :, :]
        == jnp.arange(slots, dtype=jnp.int32)[:, None, None],
        axis=2,
    ).astype(jnp.bfloat16)
    outgoing = (
        jnp.dot(dispatch, expert_hidden, preferred_element_type=jnp.float32)
        .astype(jnp.bfloat16)
        .reshape(experts, capacity, expert_hidden.shape[1] // 128, 128)
    )
    wide_turn = jnp.pad(key_turn, ((0, 0), (0, 128 - ROPE)))
    latents, turned, qlat, received = exchange((key_lat, wide_turn, query_lat), outgoing)
    count = groups * tok_rows
    latents = latents.reshape(count, latents.shape[2])
    qlat = qlat.reshape(count, qlat.shape[2])
    turned = turned[:, :, :ROPE].reshape(2, 4, 4, 16, ROPE).transpose(0, 3, 2, 1, 4)
    turned = turned.reshape(2, 16, 4 * 4 * ROPE)
    all_cos, all_sin = turn_tables(group_base + jnp.arange(count, dtype=jnp.int32), ROPE)
    width = expert_hidden.shape[1]
    mats = (
        key_plain,
        value_up,
        query_plain,
        query_rotary,
        gate_proj[0],
        up_proj[0],
        down_proj[0],
    )
    attended, sums = core(
        received.reshape(slots, width), latents, qlat, turned, mats, all_cos.T, all_sin.T
    )
    mixed = lax.dot_general(
        attended, output_proj, (((0,), (0,)), ((), ())), preferred_element_type=jnp.float32
    ).astype(jnp.bfloat16)
    mixer_out, back_rows = finish(
        mixed.reshape(groups, tok_rows, width),
        mixed_gain,
        sums.reshape(experts, capacity, width // 128, 128),
    )
    back_rows = back_rows.reshape(slots, width // 128, 128)
    picked = back_rows[target].astype(jnp.float32).reshape(tok_rows, topk, width // 128, 128)
    combined = jnp.sum(picked * route_weight[:, :, None, None], axis=1).reshape(tok_rows, width)
    expert_out = norm_rows(combined, expert_gain).astype(jnp.bfloat16)
    return (mixer_out, expert_out)


def solution(mesh):
    in_specs = (
        P(("ep", "tp"), None),
        P(("ep", "tp"), None),
        P(),
        P(),
        P(),
        P(),
        P(),
        P(),
        P(None, "tp"),
        P(None, "tp"),
        P(None, "tp"),
        P(None, "tp"),
        P("tp", None),
        P(),
        P(),
        P(("ep", "tp"), None),
        P(("ep", "tp"), None),
        P("ep", None, "tp"),
        P("ep", None, "tp"),
        P("ep", "tp", None),
        P(),
    )
    out_specs = (P(("ep", "tp"), None), P(("ep", "tp"), None))
    return jax.shard_map(
        on_device, mesh=mesh, in_specs=in_specs, out_specs=out_specs, check_vma=False
    )
```

```python
import functools

import jax
import jax.numpy as jnp
from jax import lax
from jax.experimental import pallas as pl
from jax.experimental.pallas import tpu as pltpu
from jax.sharding import PartitionSpec as P

NOPE = 64
ROPE = 32
VDIM = 64


EPS = 1e-06
CLAMP = 7.0
ALPHA = 1.702
THETA = 10000.0
FLOOR = -1e30
LOG2E = 1.4426950408889634
C = (NOPE + ROPE) ** (-0.5) * LOG2E
SUB = 64

MESH = pl.DeviceIdType.MESH
ANY = pl.BlockSpec(memory_space=pl.ANY)
HBM = pl.BlockSpec(memory_space=pltpu.HBM)
VMEM = pl.BlockSpec(memory_space=pltpu.VMEM)
DMA = pltpu.SemaphoreType.DMA


def ring_places():
    ep, tp, n = lax.axis_index("ep"), lax.axis_index("tp"), lax.axis_size("tp")
    right = lax.rem(tp + 1, n)
    left = lax.rem(tp + n - 1, n)
    across = lax.rem(tp + 2, n)
    return ep, tp, right, left, across


def partner(ep, r):
    for bit in range(r.bit_length()):
        if r >> bit & 1:
            ep = ep + (1 - 2 * lax.rem(ep // (1 << bit), 2)) * (1 << bit)
    return ep


def greet(places):
    barrier = pltpu.get_barrier_semaphore()
    for place in places:
        pl.semaphore_signal(barrier, inc=1, device_id=place, device_id_type=MESH)
    pl.semaphore_wait(barrier, len(places))


def remote(src, dst, sends, recvs, k, place):
    return pltpu.make_async_remote_copy(
        src_ref=src,
        dst_ref=dst,
        send_sem=sends.at[k],
        recv_sem=recvs.at[k],
        device_id=place,
        device_id_type=MESH,
    )


class Latents:
    def __init__(self, mine, outs, sends, recvs):
        ep, tp, right, left, across = ring_places()
        places = ((ep, right), (ep, left))
        self.mine, self.outs, self.tp = mine, outs, tp
        self.news, self.passed = [], []
        for k, (src, out) in enumerate(zip(mine, outs)):
            half = src.shape[0] // 2
            at = [pl.ds(part * half, half) for part in range(2)]
            self.news.append(
                {
                    (part, way): remote(
                        src.at[at[part]],
                        out.at[tp, at[part]],
                        sends,
                        recvs,
                        6 * k + 2 * way + part,
                        places[way],
                    )
                    for part in range(2)
                    for way in range(2)
                }
            )
            self.passed.append(
                [
                    remote(
                        out.at[(left, right)[way], at[way]],
                        out.at[(left, right)[way], at[way]],
                        sends,
                        recvs,
                        6 * k + 4 + way,
                        places[way],
                    )
                    for way in range(2)
                ]
            )

    def early(self, k):
        self.news[k][0, 0].start()
        self.news[k][1, 1].start()

    def late(self, k):
        self.news[k][1, 0].start()
        self.news[k][0, 1].start()

    def relay(self, k):
        for way in range(2):
            self.news[k][way, way].wait_recv()
            self.passed[k][way].start()

    def arrived(self, k):
        self.news[k][1, 0].wait_recv()
        self.news[k][0, 1].wait_recv()
        for copy in self.passed[k]:
            copy.wait_recv()

    def close(self):
        for news, passed in zip(self.news, self.passed):
            for copy in list(news.values()) + passed:
                copy.wait_send()


KV_ORDER = (
    [(f, 0, 0, p) for p in range(2) for f in range(2)]
    + [(f, a, 0, p) for p in range(2) for f in range(2) for a in (3, 1)]
    + [(f, 0, b, p) for p in range(2) for f in range(2) for b in (3, 1)]
    + [(f, 2, 0, p) for p in range(2) for f in range(2)]
    + [(f, 3, b, p) for p in range(2) for f in range(2) for b in (3, 1)]
    + [(f, 1, b, p) for p in range(2) for f in range(2) for b in (3, 1)]
    + [(f, 0, 2, p) for p in range(2) for f in range(2)]
    + [(f, 2, b, p) for p in range(2) for f in range(2) for b in (3, 1)]
    + [(f, a, 2, p) for a in (3, 1, 2) for p in range(2) for f in range(2)]
)
KV_SLOT = {key: k for k, key in enumerate(KV_ORDER)}

OWN, LEFT, RIGHT, FAR = range(4)
ROW_ORDER = (
    [(OWN, 0), (OWN, 1), (LEFT, 0), (RIGHT, 2), (LEFT, 1), (RIGHT, 3), (FAR, 0), (FAR, 2)]
    + [(RIGHT, 0), (LEFT, 2), (FAR, 1), (FAR, 3), (RIGHT, 1), (LEFT, 3), (OWN, 2), (OWN, 3)]
)
GROUP_OF = (0, 3, 1, 2)
CHUNK_OF = (0, 2, 3, 1)
ROW_SLOT = {key: k for k, key in enumerate(ROW_ORDER)}
BACK = (3, 1)


class Spread:
    def __init__(self, held, sends, recvs):
        ep, tp = lax.axis_index("ep"), lax.axis_index("tp")
        side = 4
        core = lax.rem(ep, 2)
        y = lax.rem(ep // 2, side)
        z = ep // (2 * side)
        self.held, self.sends, self.recvs = held, sends, recvs
        self.mate = (ep + 1 - 2 * core, tp)
        cut = held.shape[1] // 32 * 16
        self.parts = (pl.ds(0, cut), pl.ds(cut, held.shape[1] - cut))

        def index(dz, dy):
            return ((lax.rem(z + dz, side) * side + lax.rem(y + dy, side)) * 2 + core, tp)

        around = [(index(0, 1), index(0, 3)), (index(1, 0), index(3, 0))]
        self.places = [around, around[::-1]]
        self.neighbours = [place for pair in around for place in pair] + [self.mate]

    def copy(self, f, here, there, place, k, part=None):
        src = self.held.at[KV_SLOT[(f, *here)]]
        dst = self.held.at[KV_SLOT[(f, *there)]]
        if part is not None:
            src, dst = src.at[self.parts[part]], dst.at[self.parts[part]]
        return remote(src, dst, self.sends, self.recvs, 36 * f + k, place)

    def first(self, f, way):
        return self.copy(f, (0, 0, 0), (BACK[way], 0, 0), self.places[f][0][way], way)

    def first_on(self, f, way):
        return self.copy(
            f, (BACK[way], 0, 0), (2, 0, 0), self.places[f][0][way], 2 + way, part=way
        )

    def second(self, f, a, way):
        return self.copy(f, (a, 0, 0), (a, BACK[way], 0), self.places[f][1][way], 4 + 4 * a + way)

    def second_on(self, f, a, way):
        return self.copy(
            f, (a, BACK[way], 0), (a, 2, 0), self.places[f][1][way], 6 + 4 * a + way, part=way
        )

    def share(self, f, a, b):
        return self.copy(f, (a, b, 0), (a, b, 1), self.mate, 20 + 4 * a + b)

    def start(self):
        for f in range(2):
            for way in range(2):
                self.first(f, way).start()
        for f in range(2):
            self.share(f, 0, 0).start()
            for way in range(2):
                self.second(f, 0, way).start()

    def got_first(self):
        for f in range(2):
            for way in range(2):
                self.first(f, way).wait_recv()
                self.first_on(f, way).start()
                a = BACK[way]
                for there in range(2):
                    self.second(f, a, there).start()
                self.share(f, a, 0).start()

    def got_second(self, a):
        for f in range(2):
            for way in range(2):
                self.second(f, a, way).wait_recv()
                self.second_on(f, a, way).start()
                self.share(f, a, BACK[way]).start()

    def got_far_first(self):
        for f in range(2):
            for way in range(2):
                self.first_on(f, way).wait_recv()
            for there in range(2):
                self.second(f, 2, there).start()
            self.share(f, 2, 0).start()

    def got_far_second(self, a):
        for f in range(2):
            for way in range(2):
                self.second_on(f, a, way).wait_recv()
            self.share(f, a, 2).start()

    def got_shares(self, *spots):
        for f in range(2):
            for a, b in spots:
                self.share(f, a, b).wait_recv()

    def close(self):
        for f in range(2):
            for a in range(4):
                for b in range(4):
                    self.share(f, a, b).wait_send()
            for way in range(2):
                self.first(f, way).wait_send()
                self.first_on(f, way).wait_send()
                for a in range(4):
                    self.second(f, a, way).wait_send()
                    self.second_on(f, a, way).wait_send()


class Ring:
    def __init__(self, rows, sends, recvs):
        ep, tp, right, left, across = ring_places()
        self.places = ((ep, right), (ep, left))
        self.news, self.passed, self.own = {}, [], []
        for c in range(4):
            chunk = rows.at[ROW_SLOT[OWN, c]]
            for way in range(2):
                origin = (LEFT, RIGHT)[way]
                self.news[c, way] = remote(
                    chunk, rows.at[ROW_SLOT[origin, c]], sends, recvs, 4 * way + c, self.places[way]
                )
            way = c // 2
            origin = (LEFT, RIGHT)[way]
            self.passed.append(
                remote(
                    rows.at[ROW_SLOT[origin, c]],
                    rows.at[ROW_SLOT[FAR, c]],
                    sends,
                    recvs,
                    8 + c,
                    self.places[way],
                )
            )

    def start(self, c):
        self.news[c, c // 2].start()

    def relay(self, c):
        self.news[c, 0].wait_recv()
        self.passed[c].start()
        self.news[2 + c, 0].start()
        self.news[2 + c, 1].wait_recv()
        self.passed[2 + c].start()
        self.news[c, 1].start()

    def arrived(self, whose, c):
        if whose == FAR:
            self.passed[c].wait_recv()
        elif whose in (LEFT, RIGHT) and c // 2 != whose - LEFT:
            self.news[c, whose - LEFT].wait_recv()

    def close(self):
        for copy in self.passed + list(self.news.values()):
            copy.wait_send()


class Fold:
    def __init__(self, part, far, near, mixed, sends, recvs):
        self.part, self.far, self.near, self.mixed = part, far, near, mixed
        ep, tp, right, left, across = ring_places()
        self.places = ((ep, right), (ep, left))
        self.hops, self.plain, self.joined = [], [], []
        for c in range(4):
            way = c // 2
            other = 1 - way
            self.hops.append(remote(part(FAR, c), far.at[c], sends, recvs, c, self.places[way]))
            self.plain.append(
                remote(
                    part((RIGHT, LEFT)[other], c), near.at[c], sends, recvs, 4 + c, self.places[other]
                )
            )
            self.joined.append(
                remote(mixed.at[c], far.at[4 + c], sends, recvs, 8 + c, self.places[way])
            )

    def join(self, c):
        own = self.part((RIGHT, LEFT)[c // 2], c)[...]
        self.mixed[c] = (own.astype(jnp.float32) + self.far[c].astype(jnp.float32)).astype(
            jnp.bfloat16
        )

    def total(self, c):
        self.joined[c].wait_recv()
        own = self.part(OWN, c)[...].astype(jnp.float32)
        return own + self.near[c].astype(jnp.float32) + self.far[4 + c].astype(jnp.float32)

    def close(self):
        for copy in self.hops + self.plain + self.joined:
            copy.wait_send()


def fold_scratch(rows, width):
    return [
        pltpu.VMEM((8, rows // 4, width), jnp.bfloat16),
        pltpu.VMEM((4, rows // 4, width), jnp.bfloat16),
        pltpu.VMEM((4, rows // 4, width), jnp.bfloat16),
        DMA((12,)),
        DMA((12,)),
    ]


def finish_kernel(part, gain, rows, out, rows_out, kept, own_sem, far, near, mixed, sends, recvs, row_sends, row_recvs):
    ep, tp, right, left, across = ring_places()
    peers = rows.shape[0]
    swaps = [(partner(ep, r), tp) for r in range(1, peers)]
    barrier = pltpu.get_barrier_semaphore()
    for place in swaps:
        pl.semaphore_signal(barrier, inc=1, device_id=place, device_id_type=MESH)
    size = part.shape[1] // 4

    def piece(whose, c):
        return part.at[(tp, left, right, across)[whose], pl.ds(c * size, size)]

    fold = Fold(piece, far, near, mixed, sends, recvs)
    for place in fold.places:
        pl.semaphore_signal(barrier, inc=1, device_id=place, device_id_type=MESH)
    pl.semaphore_wait(barrier, len(swaps) + 2)
    for c in (0, 2, 1, 3):
        fold.hops[c].start()
    for c in (2, 0, 3, 1):
        fold.plain[c].start()
    moves = [
        remote(rows.at[r], rows_out.at[r], row_sends, row_recvs, r - 1, swaps[r - 1])
        for r in range(1, peers)
    ]
    for copy in moves:
        copy.start()
    take = pltpu.make_async_copy(rows.at[0], kept, own_sem.at[0])
    take.start()
    take.wait()
    put = pltpu.make_async_copy(kept, rows_out.at[0], own_sem.at[0])
    put.start()
    for c in (0, 2):
        fold.hops[c].wait_recv()
        fold.join(c)
    for c in (1, 3):
        fold.hops[c].wait_recv()
    for c in (0, 2):
        fold.joined[c].start()
    for c in (1, 3):
        fold.join(c)
    for c in (0, 2):
        fold.plain[c].wait_recv()
    for c in (1, 3):
        fold.joined[c].start()
        fold.plain[c].wait_recv()
    for c in range(4):
        whole = fold.total(c)
        scale = lax.rsqrt(jnp.mean(whole * whole, axis=-1, keepdims=True) + EPS)
        out[c * size : (c + 1) * size, :] = (whole * scale * gain[...]).astype(jnp.bfloat16)
    fold.close()
    for copy in moves:
        copy.wait()
    put.wait()


def finish(part, gain, rows):
    groups, count, width = part.shape
    peers = rows.shape[0]
    return pl.pallas_call(
        finish_kernel,
        out_shape=[
            jax.ShapeDtypeStruct((count, width), jnp.bfloat16),
            jax.ShapeDtypeStruct(rows.shape, rows.dtype),
        ],
        in_specs=[VMEM, VMEM, ANY],
        out_specs=[VMEM, ANY],
        scratch_shapes=[pltpu.VMEM(rows.shape[1:], rows.dtype), DMA((1,))]
        + fold_scratch(count, width)
        + [DMA((peers - 1,)), DMA((peers - 1,))],
        compiler_params=pltpu.CompilerParams(
            collective_id=3, has_side_effects=True, vmem_limit_bytes=16 * 1024 * 1024
        ),
        cost_estimate=pl.CostEstimate(flops=10**10, bytes_accessed=10**6, transcendentals=0),
    )(part, gain.reshape(1, width), rows)


def core_kernel(
    key_lat,
    wide_turn,
    hidden_in,
    query_down,
    query_gain,
    outgoing,
    key_plain_in,
    value_up_in,
    query_plain_in,
    query_rotary_in,
    gate_in,
    up_in,
    down_in,
    cosine,
    sine,
    o_ref,
    sum_ref,
    rhs,
    s_buf,
    p_buf,
    peak,
    acc,
    held,
    rows,
    part,
    latents,
    turned,
    qlat,
    key_plain,
    value_up,
    query_plain,
    query_rotary,
    gate_w,
    up_w,
    down_w,
    hidden,
    load_sem,
    lat_sends,
    lat_recvs,
    swap_sends,
    swap_recvs,
    row_sends,
    row_recvs,
    kv_sends,
    kv_recvs,
    *fold_refs,
):
    step = pl.program_id(0)
    heads = acc.shape[0]
    pair = 4
    wide = held.shape[2]
    size = wide // 2
    subs = size // SUB
    count = pair * SUB
    queries = o_ref.shape[1]
    chunk_rows, pieces = rows.shape[1], rows.shape[2]
    peers, slots_each = outgoing.shape[0], outgoing.shape[1]
    ep, tp = lax.axis_index("ep"), lax.axis_index("tp")
    spread = Spread(held, kv_sends, kv_recvs)
    ring = Ring(rows, row_sends, row_recvs)
    fold = Fold(lambda whose, c: part.at[ROW_SLOT[whose, c]], *fold_refs)
    lat = Latents(
        (key_lat, wide_turn, qlat.at[tp]), (latents, turned, qlat), lat_sends, lat_recvs
    )
    swaps = [(partner(ep, r), tp) for r in range(1, peers)]
    group = peers // 4

    def spot(r):
        return rows.at[ROW_SLOT[OWN, CHUNK_OF[r // group]], pl.ds(r % group * slots_each, slots_each)]

    moves = [
        remote(outgoing.at[r], spot(r), swap_sends, swap_recvs, r - 1, swaps[r - 1])
        for r in range(1, peers)
    ]
    loads = [
        pltpu.make_async_copy(src, dst, load_sem.at[k])
        for k, (src, dst) in enumerate(
            [
                (key_lat, latents.at[tp]),
                (wide_turn, turned.at[tp]),
                (key_plain_in, key_plain),
                (value_up_in, value_up),
                (outgoing.at[0], spot(0)),
                (query_plain_in, query_plain),
                (query_rotary_in, query_rotary),
                (gate_in, gate_w),
                (up_in, up_w),
                (down_in, down_w),
            ]
        )
    ]

    deep, broad = query_down.shape[0] // 256, query_down.shape[1] // queries
    tiles = [rhs.at[k // 4, k % 4] for k in range(16)]
    tiles += [p_buf.at[k // 4, pl.ds(k % 4 * 256, 256)] for k in range(8)]
    tiles = tiles[: deep * broad]
    weights = [pltpu.make_async_copy(hidden_in, hidden, load_sem.at[10])] + [
        pltpu.make_async_copy(
            query_down.at[pl.ds(256 * (k % deep), 256), pl.ds(queries * (k // deep), queries)],
            tile,
            load_sem.at[11 + k],
        )
        for k, tile in enumerate(tiles)
    ]

    def make_query_latents():
        for copy in weights:
            copy.wait()
        blocks = []
        for n in range(broad):
            total = None
            for k in range(deep):
                term = jnp.dot(
                    hidden[:, 256 * k : 256 * (k + 1)],
                    tiles[n * deep + k][...],
                    preferred_element_type=jnp.float32,
                )
                total = term if total is None else total + term
            blocks.append(total)
        whole = jnp.concatenate(blocks, axis=1)
        scale = lax.rsqrt(jnp.mean(whole * whole, axis=-1, keepdims=True) + EPS)
        qlat[tp] = (whole * scale * query_gain[...]).astype(jnp.bfloat16)

    def make_keys():
        both = latents[...].reshape(queries, latents.shape[2])
        keys = jnp.dot(both, key_plain[...], preferred_element_type=jnp.float32)
        values = jnp.dot(both, value_up[...], preferred_element_type=jnp.float32).T
        keys, values = keys.astype(jnp.bfloat16), values.astype(jnp.bfloat16)
        half = size // 2
        for f in range(2):
            own = KV_SLOT[f, 0, 0, 0]
            held[own, :half, :size] = keys[size * f : size * f + half]
            held[own, :half, size:] = keys[size * f + half : size * f + size]
            held[own, half:size, :size] = values[:half, size * f : size * f + size]
            held[own, half:size, size:] = values[half:, size * f : size * f + size]
            turns = (
                turned[2 * f, :SUB]
                + turned[2 * f, SUB:]
                + turned[2 * f + 1, :SUB]
                + turned[2 * f + 1, SUB:]
            )
            tall = held.shape[1] - size
            for g in range(SUB // tall):
                held[own, size:, g * 128 : (g + 1) * 128] = turns[g * tall : (g + 1) * tall]

    def make_queries():
        both = qlat[...].reshape(queries, qlat.shape[2])
        plain = jnp.dot(both, query_plain[...], preferred_element_type=jnp.float32)
        plain = plain.T.astype(jnp.bfloat16)
        rotated = jnp.dot(both, query_rotary[...], preferred_element_type=jnp.float32).T
        quarter = ROPE // 2
        for h in range(heads):
            a = rotated[h * ROPE : h * ROPE + quarter]
            b = rotated[h * ROPE + quarter : h * ROPE + ROPE]
            first = (a * cosine[...] - b * sine[...]).astype(jnp.bfloat16)
            second = (b * cosine[...] + a * sine[...]).astype(jnp.bfloat16)
            at = h % 2 * NOPE
            for j in range(subs):
                rhs[h, j, at : at + NOPE, :] = plain[h * NOPE : (h + 1) * NOPE]
                low = 128 + j * ROPE
                rhs[h, j, low : low + quarter, :] = first
                rhs[h, j, low + quarter : low + ROPE, :] = second

    def collect(c):
        g = GROUP_OF[c]
        for r in range(max(1, g * group), (g + 1) * group):
            moves[r - 1].wait_recv()
        ring.start(c)

    @pl.when(step == 0)
    def _():
        barrier = pltpu.get_barrier_semaphore()
        places = list(ring.places) + swaps
        for place in places:
            pl.semaphore_signal(barrier, inc=1, device_id=place, device_id_type=MESH)
        for copy in weights + loads:
            copy.start()
        peak[...] = jnp.full_like(peak, FLOOR)
        acc[...] = jnp.zeros_like(acc)
        pl.semaphore_wait(barrier, len(places))
        for k in range(2):
            lat.early(k)
            lat.late(k)
        for g in (0, 1, 3, 2):
            for r in range(max(1, g * group), (g + 1) * group):
                moves[r - 1].start()
        make_query_latents()
        rhs[...] = jnp.zeros_like(rhs)
        for k in range(2):
            lat.relay(k)
        lat.early(2)
        lat.late(2)
        for copy in loads[:5]:
            copy.wait()
        for k in range(2):
            lat.arrived(k)
        make_keys()
        lat.relay(2)
        spread.start()
        collect(0)
        collect(2)
        for copy in loads[5:7]:
            copy.wait()
        lat.arrived(2)
        make_queries()
        collect(1)
        collect(3)
        for copy in loads[7:]:
            copy.wait()
        spread.got_first()
        spread.got_shares((0, 0))

    def expert(k):
        both = 2 * chunk_rows
        piece = rows[pl.ds(2 * k, 2)].reshape(both, pieces * 128)
        gate = jnp.minimum(jnp.dot(piece, gate_w[...], preferred_element_type=jnp.float32), CLAMP)
        up = jnp.clip(jnp.dot(piece, up_w[...], preferred_element_type=jnp.float32), -CLAMP, CLAMP)
        acts = ((up + 1.0) * gate * jax.nn.sigmoid(ALPHA * gate)).astype(jnp.bfloat16)
        result = jnp.dot(acts, down_w[...], preferred_element_type=jnp.float32)
        part[pl.ds(2 * k, 2)] = result.astype(jnp.bfloat16).reshape(2, chunk_rows, -1)

    def shares(*spots):
        return lambda: spread.got_shares(*spots)

    def second(a):
        return lambda: spread.got_second(a)

    def far_second(a):
        return lambda: spread.got_far_second(a)

    def join(c):
        def run():
            fold.hops[c].wait_recv()
            fold.join(c)

        return run

    plan = {
        1: [lambda: ring.relay(0)],
        2: [shares((3, 0), (1, 0)), lambda: ring.relay(1)],
        3: [second(0)],
        4: [shares((0, 3), (0, 1)), lambda: spread.got_far_first()],
        5: [fold.hops[0].start, fold.hops[2].start, shares((2, 0)), second(3)],
        6: [fold.plain[2].start, fold.plain[0].start, second(1)],
        7: [shares((3, 3), (3, 1)), second(2)],
        8: [far_second(0)],
        9: [fold.hops[1].start, fold.hops[3].start, shares((1, 3), (1, 1)), far_second(3)],
        10: [fold.plain[3].start, fold.plain[1].start, shares((0, 2)), far_second(1)],
        11: [join(0), join(2), far_second(2)],
        12: [fold.joined[0].start, fold.joined[2].start, shares((2, 3), (2, 1))],
        13: [shares((3, 2))],
        14: [shares((1, 2)), join(1), join(3)],
        15: [fold.joined[1].start, fold.joined[3].start, shares((2, 2))],
    }
    work = {0: 0, 1: 1, 2: 2, 4: 3, 6: 4, 8: 5, 10: 6, 12: 7}
    for k in range(16):

        @pl.when(step == k)
        def _(k=k):
            for action in plan.get(k, ()):
                action()
            if k in work:
                for key in ROW_ORDER[2 * work[k] : 2 * work[k] + 2]:
                    ring.arrived(*key)

    @pl.when((step <= 2) | ((step <= 12) & (lax.rem(step, 2) == 0)))
    def _():
        expert(jnp.where(step <= 2, step, 1 + step // 2))

    kv_ref = held.at[pl.ds(pair * step, pair)]
    turns = jnp.concatenate(
        [kv_ref[b, size:, g * 128 : (g + 1) * 128] for b in range(pair) for g in range(wide // 128)],
        axis=0,
    )

    def scores(h):
        half = size // 2
        best = None
        for j in range(subs):
            at = j * SUB % half
            lanes = j * SUB // half * size + h // 2 * 128
            left = jnp.concatenate(
                [kv_ref[b, at : at + SUB, lanes : lanes + 128] for b in range(pair)], axis=0
            )
            left = jnp.concatenate([left, turns], axis=1)
            block = jnp.dot(left, rhs[h, j], preferred_element_type=jnp.float32)
            for b in range(pair):
                s_buf[h % 2, b * size + j * SUB : b * size + (j + 1) * SUB, :] = block[
                    b * SUB : (b + 1) * SUB
                ]
            top = jnp.max(block.reshape(count // 8, 8, queries), axis=0)
            best = top if best is None else jnp.maximum(best, top)
        return jnp.max(best, axis=0, keepdims=True)

    def finish(h, best):
        old = peak[h : h + 1, :]
        new = jnp.maximum(old, best)
        peak[h : h + 1, :] = new
        shrink = jnp.exp2((old - new) * C)
        base = new * C
        for b in range(pair):
            at = slice(b * size, (b + 1) * size)
            p_buf[h % 2, at, :] = jnp.exp2(s_buf[h % 2, at, :] * C - base).astype(jnp.bfloat16)
        half = size // 2
        at = h * VDIM % half
        lanes = h * VDIM // half * size
        left = jnp.concatenate(
            [
                kv_ref[b, half + at : half + at + VDIM, lanes : lanes + size]
                for b in range(pair)
            ],
            axis=1,
        )
        left = jnp.concatenate([left, jnp.ones((16, left.shape[1]), jnp.bfloat16)], axis=0)
        more = jnp.dot(left, p_buf[h % 2], preferred_element_type=jnp.float32)
        acc[h] = acc[h] * shrink + more

    best = scores(0)
    for h in range(heads):
        later = scores(h + 1) if h + 1 < heads else None
        finish(h, best)
        best = later

    @pl.when(step == pl.num_programs(0) - 1)
    def _():
        for h in range(heads):
            o_ref[h * VDIM : (h + 1) * VDIM, :] = (
                acc[h, :VDIM, :] / acc[h, VDIM : VDIM + 1, :]
            ).astype(jnp.bfloat16)
        for c in range(4):
            fold.plain[c].wait_recv()
            at = GROUP_OF[c] * chunk_rows
            sum_ref[at : at + chunk_rows, :] = fold.total(c).astype(jnp.bfloat16)
        fold.close()
        ring.close()
        spread.close()
        lat.close()
        for copy in moves:
            copy.wait_send()


def core(key_lat, wide_turn, hidden, query_down, query_gain, outgoing, mats, cosine, sine):
    key_plain, value_up, query_plain, query_rotary, gate_w, up_w, down_w = mats
    heads = query_plain.shape[1] // NOPE
    groups = lax.axis_size("tp")
    queries = groups * key_lat.shape[0]
    size = key_plain.shape[1]
    wide = 2 * size
    height = size + SUB // 4
    peers, capacity, pieces, _ = outgoing.shape
    slots, width = peers * capacity, pieces * 128
    subs = size // SUB
    bf16 = jnp.bfloat16
    return pl.pallas_call(
        core_kernel,
        out_shape=[
            jax.ShapeDtypeStruct((heads * VDIM, queries), bf16),
            jax.ShapeDtypeStruct((slots, width), bf16),
        ],
        grid=(16,),
        in_specs=[HBM] * 4 + [VMEM] + [HBM] * 8 + [VMEM] * 2,
        out_specs=[VMEM, VMEM],
        scratch_shapes=[
            pltpu.VMEM((heads, subs, 256, queries), bf16),
            pltpu.VMEM((2, 4 * size, queries), jnp.float32),
            pltpu.VMEM((2, 4 * size, queries), bf16),
            pltpu.VMEM((8, queries), jnp.float32),
            pltpu.VMEM((heads, VDIM + 16, queries), jnp.float32),
            pltpu.VMEM((64, height, wide), bf16),
            pltpu.VMEM((16, slots // 4, pieces, 128), bf16),
            pltpu.VMEM((16, slots // 4, width), bf16),
        ]
        + [pltpu.VMEM((groups, *a.shape), bf16) for a in (key_lat, wide_turn)]
        + [pltpu.VMEM((groups, key_lat.shape[0], query_down.shape[1]), bf16)]
        + [pltpu.VMEM(a.shape, bf16) for a in mats]
        + [pltpu.VMEM(hidden.shape, bf16)]
        + [DMA((n,)) for n in (35, 18, 18, peers - 1, peers - 1, 12, 12, 72, 72)]
        + fold_scratch(slots, width),
        compiler_params=pltpu.CompilerParams(
            dimension_semantics=("arbitrary",),
            vmem_limit_bytes=63 * 1024 * 1024,
            collective_id=4,
            has_side_effects=True,
        ),
        cost_estimate=pl.CostEstimate(flops=10**11, bytes_accessed=10**7, transcendentals=10**7),
    )(
        key_lat,
        wide_turn,
        hidden,
        query_down,
        query_gain.reshape(1, -1),
        outgoing,
        *mats,
        cosine,
        sine,
    )


def norm_rows(values, gain):
    values = values.astype(jnp.float32)
    scale = lax.rsqrt(jnp.mean(values * values, axis=-1, keepdims=True) + EPS)
    return values * scale * gain


def turn_tables(positions, width):
    half = width // 2
    freqs = THETA ** (-2.0 * jnp.arange(half, dtype=jnp.float32) / width)
    angles = positions.astype(jnp.float32)[:, None] * freqs[None, :]
    return (jnp.cos(angles), jnp.sin(angles))


def rotate(values, cosine, sine):
    half = values.shape[-1] // 2
    first = values[..., :half]
    second = values[..., half:]
    return jnp.concatenate(
        [first * cosine - second * sine, second * cosine + first * sine], axis=-1
    )


def on_device(
    mixer_input,
    expert_input,
    mixer_gain,
    query_down,
    latent_down,
    rotary_down,
    query_gain,
    latent_gain,
    query_plain,
    query_rotary,
    key_plain,
    value_up,
    output_proj,
    mixed_gain,
    expert_norm,
    route_ids,
    route_weight,
    gate_proj,
    up_proj,
    down_proj,
    expert_gain,
):
    tok_rows = mixer_input.shape[0]
    groups = lax.axis_size("tp")
    group_base = lax.axis_index("ep") * groups * tok_rows
    offset = group_base + lax.axis_index("tp") * tok_rows
    hidden = norm_rows(mixer_input, mixer_gain).astype(jnp.bfloat16)
    key_lat = norm_rows(
        jnp.dot(hidden, latent_down, preferred_element_type=jnp.float32), latent_gain
    ).astype(jnp.bfloat16)
    cosine, sine = turn_tables(offset + jnp.arange(tok_rows, dtype=jnp.int32), ROPE)
    key_turn = rotate(
        jnp.dot(hidden, rotary_down, preferred_element_type=jnp.float32), cosine, sine
    ).astype(jnp.bfloat16)
    expert_hidden = norm_rows(expert_input, expert_norm).astype(jnp.bfloat16)
    experts = lax.axis_size("ep")
    topk = route_ids.shape[1]
    capacity = 5 * tok_rows * topk // (4 * experts)
    slots = experts * capacity
    flat_ids = route_ids.reshape(-1)
    onehot = (flat_ids[:, None] == jnp.arange(experts, dtype=jnp.int32)[None, :]).astype(jnp.int32)
    order = jnp.sum((jnp.cumsum(onehot, axis=0) - onehot) * onehot, axis=1)
    target = (flat_ids ^ lax.axis_index("ep")) * capacity + order
    dispatch = jnp.any(
        target.reshape(tok_rows, topk)[None, :, :]
        == jnp.arange(slots, dtype=jnp.int32)[:, None, None],
        axis=2,
    ).astype(jnp.bfloat16)
    outgoing = (
        jnp.dot(dispatch, expert_hidden, preferred_element_type=jnp.float32)
        .astype(jnp.bfloat16)
        .reshape(experts, capacity, expert_hidden.shape[1] // 128, 128)
    )
    strip = lax.axis_index("tp") % 2 * 2 + jnp.arange(tok_rows, dtype=jnp.int32)[:, None] // SUB
    lane = jnp.arange(128, dtype=jnp.int32)[None, :] // ROPE
    wide_turn = jnp.where(lane == strip, jnp.tile(key_turn, (1, 128 // ROPE)), 0)
    wide_turn = wide_turn.astype(jnp.bfloat16)
    count = groups * tok_rows
    all_cos, all_sin = turn_tables(group_base + jnp.arange(count, dtype=jnp.int32), ROPE)
    width = expert_hidden.shape[1]
    mats = (
        key_plain,
        value_up,
        query_plain,
        query_rotary,
        gate_proj[0],
        up_proj[0],
        down_proj[0],
    )
    attended, sums = core(
        key_lat, wide_turn, hidden, query_down, query_gain, outgoing, mats, all_cos.T, all_sin.T
    )
    mixed = lax.dot_general(
        attended, output_proj, (((0,), (0,)), ((), ())), preferred_element_type=jnp.float32
    ).astype(jnp.bfloat16)
    mixer_out, back_rows = finish(
        mixed.reshape(groups, tok_rows, width),
        mixed_gain,
        sums.reshape(experts, capacity, width // 128, 128),
    )
    back_rows = back_rows.reshape(slots, width // 128, 128)
    picked = back_rows[target].astype(jnp.float32).reshape(tok_rows, topk, width // 128, 128)
    combined = jnp.sum(picked * route_weight[:, :, None, None], axis=1).reshape(tok_rows, width)
    expert_out = norm_rows(combined, expert_gain).astype(jnp.bfloat16)
    return (mixer_out, expert_out)


def solution(mesh):
    in_specs = (
        P(("ep", "tp"), None),
        P(("ep", "tp"), None),
        P(),
        P(),
        P(),
        P(),
        P(),
        P(),
        P(None, "tp"),
        P(None, "tp"),
        P(None, "tp"),
        P(None, "tp"),
        P("tp", None),
        P(),
        P(),
        P(("ep", "tp"), None),
        P(("ep", "tp"), None),
        P("ep", None, "tp"),
        P("ep", None, "tp"),
        P("ep", "tp", None),
        P(),
    )
    out_specs = (P(("ep", "tp"), None), P(("ep", "tp"), None))
    return jax.shard_map(
        on_device, mesh=mesh, in_specs=in_specs, out_specs=out_specs, check_vma=False
    )
```
